32 devices in a mesh: sp: 16 (over z, y, x), tp: 2 (over core).
Axes of the slice: x: 2, y: 2, z: 4, core: 2. Of those that a mesh axis runs over, the one named last changes fastest.
Arguments:
- tokens: bfloat16 [6144, 2048], P('sp', 'tp'), may hold values from -1620 to 1620
- input_norm_gain: float32 [2048], replicated, may hold values from 0.1 to 1.9
- outer_gate_weight: bfloat16 [2048, 1024], P(None, 'tp'), may hold values from -0.125 to 0.125
- inner_gate_weight: bfloat16 [2048, 1024], P(None, 'tp'), may hold values from -0.125 to 0.125
- convolution_input_weight: bfloat16 [2048, 1024], P(None, 'tp'), may hold values from -0.125 to 0.125
- convolution_kernel_taps: bfloat16 [3, 1024], P(None, 'tp'), may hold values from -3 to 3
- query_weight_matrix: bfloat16 [2048, 512], P(None, 'tp'), may hold values from -0.125 to 0.125
- key_weight_matrix: bfloat16 [2048, 512], P(None, 'tp'), may hold values from -0.125 to 0.125
- value_weight_matrix: bfloat16 [2048, 1024], P(None, 'tp'), may hold values from -0.125 to 0.125
- forget_gate_weight: bfloat16 [2048, 512], P(None, 'tp'), may hold values from -0.125 to 0.125
- attention_gate_weight: bfloat16 [2048, 1024], P(None, 'tp'), may hold values from -0.125 to 0.125
- forget_gate_bias: float32 [512], P('tp'), may hold values from -1.5 to 10
- extra_logarithm_decay: float32 [6144, 16], P('sp', 'tp'), may hold values from -0.72 to 0
- initial_head_state: float32 [16, 32, 64], P('tp'), may hold values from -768 to 768
- head_norm_gain: float32 [64], replicated, may hold values from 0.1 to 1.9
- convolution_output_weight: bfloat16 [1024, 2048], P('tp'), may hold values from -0.125 to 0.125
- attention_output_weight: bfloat16 [1024, 2048], P('tp'), may hold values from -0.125 to 0.125
Outputs:
- mixed: bfloat16 [6144, 2048], P(('sp', 'tp'))
The draws below stay inside these ranges and needn't reach their ends.
All inputs are finite; a program needn't handle non-finite values.
Results may differ from the reference program's by a relative error of at most 0.017.
Values may be sent and summed in bfloat16 or wider, within the bound.
No kernel may reach another device: no remote copies, remote signals or barrier semaphores. Data moves between devices by JAX's collectives and lax.ppermute only.
A program may use at most 128 MiB of HBM per device.

```python
import math
import jax
import jax.numpy as jnp
from jax import lax

D = 2048
CW = 1024
HEADS = 16
DK = 32
DV = 64
CONV_K = 3
BLOCK = 64
TOK_DEV = 384
TOKENS = 6144


def draw_tokens(key, part):
    noise_key, row_key, col_key = jax.random.split(jax.random.fold_in(key, 11), 3)
    noise = jax.random.truncated_normal(noise_key, -6.0, 6.0, (TOKENS, D), jnp.float32)
    row_scale = jnp.exp(jax.random.uniform(row_key, (TOKENS, 1), jnp.float32) * math.log(10.0))
    ramp = jnp.arange(D, dtype=jnp.float32) / max(D - 1, 1)
    rise = math.log(3.0)
    col_scale = jnp.exp(rise * ramp[None, :] + jax.random.uniform(col_key, (1, D), jnp.float32) * math.log(3.0))
    return (noise * row_scale * col_scale).astype(jnp.bfloat16)


def draw_forget_gate_bias(key, part):
    kind_key, slow_key, fast_key, jitter_key = jax.random.split(jax.random.fold_in(key, 23), 4)
    order = jax.random.permutation(kind_key, HEADS)
    fast_count = HEADS // 2
    is_fast = (order < fast_count)[:, None]
    slow = jax.random.uniform(slow_key, (HEADS, 1), jnp.float32, 8.0, 9.5)
    fast = jax.random.uniform(fast_key, (HEADS, 1), jnp.float32, -1.0, 1.0)
    jitter = jax.random.uniform(jitter_key, (HEADS, DK), jnp.float32, -0.5, 0.5)
    return (jnp.where(is_fast, fast, slow) + jitter).reshape(HEADS * DK)


def draw_extra_logarithm_decay(key, part):
    rate_key, hit_key, size_key = jax.random.split(jax.random.fold_in(key, 37), 3)
    device_blocks = TOKENS // TOK_DEV
    spread = jax.random.uniform(rate_key, (device_blocks, HEADS), jnp.float32) * math.log(4.0)
    per_row = jnp.repeat(5e-06 * jnp.exp(spread), TOK_DEV, axis=0)
    hits = jax.random.randint(hit_key, (TOKENS, HEADS), 0, TOKENS) < 2
    sizes = jax.random.uniform(size_key, (TOKENS, HEADS), jnp.float32, math.log(0.5), math.log(0.8))
    return -per_row + jnp.where(hits, sizes, 0.0)


def block_scale(rng, dims, pieces, least, top_value):
    gain = 1.0
    for axis_at, parts in pieces:
        heights = jax.random.uniform(jax.random.fold_in(jax.random.fold_in(rng, 6), axis_at), (parts,), jnp.float32, least / len(pieces), top_value / len(pieces))
        gain = gain * jnp.repeat(jnp.exp(heights), dims[axis_at] // parts).reshape((-1,) + (1,) * (len(dims) - 1 - axis_at))
    return gain


def bell_draw(rng, shape, deviation, most, cuts=(), kind=jnp.bfloat16):
    level = block_scale(rng, shape, cuts, -0.22, 0.18) if cuts else 1.0
    result = jax.random.normal(rng, shape, jnp.float32) * deviation * level
    return jnp.minimum(jnp.maximum(result, -most), most).astype(kind)


def setup_inputs(seed: int = 0) -> dict:
    seeds = jax.random.split(jax.random.key(seed), 18)
    return {
        "tokens": draw_tokens(jax.random.fold_in(seeds[17], 71), 0),
        "input_norm_gain": jnp.clip(1.0 + 0.18 * jax.random.normal(seeds[1], (D,), jnp.float32), 0.1, 1.9),
        "outer_gate_weight": bell_draw(seeds[2], (D, CW), D ** -0.5, 0.125, ((1, 2),)),
        "inner_gate_weight": bell_draw(seeds[3], (D, CW), D ** -0.5, 0.125, ((1, 2),)),
        "convolution_input_weight": bell_draw(seeds[4], (D, CW), D ** -0.5, 0.125, ((1, 2),)),
        "convolution_kernel_taps": bell_draw(seeds[5], (CONV_K, CW), 0.577, 3.0, ((1, 2),)),
        "query_weight_matrix": bell_draw(seeds[6], (D, HEADS * DK), D ** -0.5, 0.125, ((1, 2),)),
        "key_weight_matrix": bell_draw(seeds[7], (D, HEADS * DK), D ** -0.5, 0.125, ((1, 2),)),
        "value_weight_matrix": bell_draw(seeds[8], (D, HEADS * DV), D ** -0.5, 0.125, ((1, 2),)),
        "forget_gate_weight": bell_draw(seeds[9], (D, HEADS * DK), D ** -0.5, 0.125, ((1, 2),)),
        "attention_gate_weight": bell_draw(seeds[10], (D, HEADS * DV), D ** -0.5, 0.125, ((1, 2),)),
        "forget_gate_bias": draw_forget_gate_bias(jax.random.fold_in(seeds[17], 71), 0),
        "extra_logarithm_decay": draw_extra_logarithm_decay(jax.random.fold_in(seeds[17], 71), 0),
        "initial_head_state": bell_draw(seeds[13], (HEADS, DK, DV), 128.0, 768.0, ((0, 2),), jnp.float32),
        "head_norm_gain": jnp.clip(1.0 + 0.18 * jax.random.normal(seeds[14], (DV,), jnp.float32), 0.1, 1.9),
        "convolution_output_weight": bell_draw(seeds[15], (CW, D), (CW + HEADS * DV) ** -0.5, 0.125, ((0, 2),)),
        "attention_output_weight": bell_draw(seeds[16], (HEADS * DV, D), (CW + HEADS * DV) ** -0.5, 0.125, ((0, 2),)),
    }


NORM_EPS = 1e-06
GATE_SOFTNESS = 16.0

def block_terms(queries, key_rows, values, logarithm_decay):
    cumulative = jnp.cumsum(logarithm_decay, axis=1)
    last_log = cumulative[:, -1:]
    query_g = queries * jnp.exp(cumulative)
    key_g = key_rows * jnp.exp(-cumulative)
    scores = jnp.einsum('nihd,njhd->nhij', query_g, key_g, precision=lax.Precision.HIGHEST)
    width = queries.shape[1]
    causal = jnp.arange(width)[:, None] >= jnp.arange(width)[None, :]
    scores = jnp.where(causal, scores, 0.0)
    inner = jnp.einsum('nhij,njhe->nihe', scores, values, precision=lax.Precision.HIGHEST)
    key_decayed = key_rows * jnp.exp(last_log - cumulative)
    update = jnp.einsum('nchd,nche->nhde', key_decayed, values, precision=lax.Precision.HIGHEST)
    return (query_g, inner, update, last_log[:, 0])

def carry_step(state, inputs):
    block_decay, update = inputs
    return (block_decay[..., None] * state + update, state)

def reference(tokens, input_norm_gain, outer_gate_weight, inner_gate_weight, convolution_input_weight, convolution_kernel_taps, query_weight_matrix, key_weight_matrix, value_weight_matrix, forget_gate_weight, attention_gate_weight, forget_gate_bias, extra_logarithm_decay, initial_head_state, head_norm_gain, convolution_output_weight, attention_output_weight):
    sequence_length = tokens.shape[0]
    number_of_heads, key_channel_count, value_dim = initial_head_state.shape
    features = tokens.astype(jnp.float32)
    power = lax.optimization_barrier(jnp.mean(features * features, axis=1, keepdims=True))
    normed = (features * lax.rsqrt(power + NORM_EPS) * input_norm_gain).astype(jnp.bfloat16)

    def project(weight):
        return jnp.dot(normed, weight, preferred_element_type=jnp.float32).astype(jnp.bfloat16)
    conv_b, conv_c, conv_h = (project(outer_gate_weight), project(inner_gate_weight), project(convolution_input_weight))
    query, key_proj, value = (project(query_weight_matrix), project(key_weight_matrix), project(value_weight_matrix))
    forget_preactivation, out_gate = (project(forget_gate_weight), project(attention_gate_weight))
    product = (conv_c.astype(jnp.float32) * conv_h.astype(jnp.float32)).astype(jnp.bfloat16)
    tap_count = convolution_kernel_taps.shape[0]
    padded = jnp.concatenate([jnp.zeros((tap_count - 1, product.shape[1]), jnp.bfloat16), product], axis=0)
    conv = jnp.zeros(product.shape, jnp.float32)
    for tap_index in range(tap_count):
        conv = conv + convolution_kernel_taps[tap_index].astype(jnp.float32) * padded[tap_index:tap_index + sequence_length].astype(jnp.float32)
    conv_out = (conv_b.astype(jnp.float32) * conv).astype(jnp.bfloat16)
    logarithm_decay = jax.nn.log_sigmoid(forget_preactivation.astype(jnp.float32) + forget_gate_bias) / GATE_SOFTNESS
    logarithm_decay = logarithm_decay.reshape(sequence_length, number_of_heads, key_channel_count) + extra_logarithm_decay[:, :, None]
    n_blocks = sequence_length // BLOCK
    queries = (query.astype(jnp.float32) * key_channel_count ** (-0.5)).reshape(n_blocks, BLOCK, number_of_heads, key_channel_count)
    key_rows = key_proj.astype(jnp.float32).reshape(n_blocks, BLOCK, number_of_heads, key_channel_count)
    values = value.astype(jnp.float32).reshape(n_blocks, BLOCK, number_of_heads, value_dim)
    query_g, inner, update, block_log = block_terms(queries, key_rows, values, logarithm_decay.reshape(n_blocks, BLOCK, number_of_heads, key_channel_count))
    final_state, entering = lax.scan(carry_step, initial_head_state.astype(jnp.float32), (jnp.exp(block_log), update))
    outer = jnp.einsum('nchd,nhde->nche', query_g, entering, precision=lax.Precision.HIGHEST)
    raw = (inner + outer).reshape(sequence_length, number_of_heads, value_dim)
    raw = raw * lax.rsqrt(lax.optimization_barrier(jnp.mean(raw * raw, axis=2, keepdims=True)) + NORM_EPS) * head_norm_gain
    gate_values = jax.nn.silu(out_gate.astype(jnp.float32)).reshape(sequence_length, number_of_heads, value_dim)
    attn_out = (raw * gate_values).reshape(sequence_length, number_of_heads * value_dim).astype(jnp.bfloat16)
    mixed = jnp.dot(conv_out, convolution_output_weight, preferred_element_type=jnp.float32)
    mixed = mixed + jnp.dot(attn_out, attention_output_weight, preferred_element_type=jnp.float32)
    return mixed.astype(jnp.bfloat16)
```

```python
import functools

import jax
import jax.numpy as jnp
from jax import lax
from jax.experimental import pallas as pl
from jax.experimental.pallas import tpu as pltpu
from jax.sharding import PartitionSpec as P

BLOCK = 64
NORM_EPS = 1e-06
GATE_SOFTNESS = 16.0
F32 = jnp.float32
BF16 = jnp.bfloat16
NT = (((1,), (1,)), ((), ()))
TN = (((0,), (0,)), ((), ()))
VMEM = pl.BlockSpec(memory_space=pltpu.VMEM)
SMEM = pl.BlockSpec(memory_space=pltpu.SMEM)
HBM = pl.BlockSpec(memory_space=pl.ANY)
EXTRA_ROWS = 16


def dot(a, b):
    return jnp.dot(a, b, preferred_element_type=F32)


def call(body, outs, ins, flops, scratch=(), limit=48 << 20, name=None):
    specs = [s for _, s in ins]
    return pl.pallas_call(
        body,
        out_shape=[jax.ShapeDtypeStruct(s, d) for s, d in outs],
        in_specs=specs,
        out_specs=[VMEM] * len(outs),
        scratch_shapes=list(scratch),
        compiler_params=pltpu.CompilerParams(vmem_limit_bytes=limit),
        cost_estimate=pl.CostEstimate(flops=flops, bytes_accessed=1 << 20, transcendentals=0),
        name=name,
    )(*[a for a, _ in ins])


def weight_copies(hbm, buf, sems, row, rows):
    copies, at = [], 0
    for i, w in enumerate(hbm):
        cols = w.shape[1]
        copies.append(
            pltpu.make_async_copy(
                w.at[pl.ds(row, rows), :], buf.at[:, at : at + cols], sems.at[i]
            )
        )
        at += cols
    return copies


def tile_lanes(column, lanes):
    return jnp.concatenate([column] * (lanes // column.shape[1]), axis=1)


def block_mask(rows, row_step, lanes, lane_step):
    r = lax.broadcasted_iota(jnp.int32, (rows, lanes), 0) // row_step
    c = lax.broadcasted_iota(jnp.int32, (rows, lanes), 1) // lane_step
    return r == c


def own_half(tp, tok, gain, extra, *refs):
    weights, (acc, xg, ssq, wide), (buf, sems) = refs[:5], refs[5:9], refs[9:]
    half = tok.shape[1]
    at = pl.multiple_of(tp[0] * half, half)
    copies = weight_copies(weights, buf, sems, at, half)
    for c in copies:
        c.start()
    x = tok[...].astype(F32)
    ssq[...] = jnp.broadcast_to(jnp.sum(x * x, axis=1, keepdims=True), ssq.shape)
    xg[...] = (x * gain[:, pl.ds(at, half)]).astype(BF16)
    heads = extra.shape[1]
    lanes = wide.shape[1]
    r = lax.broadcasted_iota(jnp.int32, (heads, lanes), 0)
    c = lax.broadcasted_iota(jnp.int32, (heads, lanes), 1) // (lanes // heads)
    wide[...] = jnp.dot(
        extra[...],
        (r == c).astype(F32),
        precision=lax.Precision.HIGHEST,
        preferred_element_type=F32,
    )
    left = xg[...]
    at = 0
    for c, w in zip(copies, weights):
        cols = w.shape[1]
        c.wait()
        acc[:, at : at + cols] = dot(left, buf[:, at : at + cols])
        at += cols


def other_half(tp, tok, gain, bias, acc, xg, ssq, wide, *refs):
    weights = refs[:5]
    full, scale, key, val, cum, base, prod, own, send = refs[5:14]
    buf, sems = refs[14:]
    rows, half = tok.shape
    at = pl.multiple_of((1 - tp[0]) * half, half)
    copies = weight_copies(weights, buf, sems, at, half)
    for c in copies:
        c.start()
    x = tok[...].astype(F32)
    power = (ssq[:, :1] + jnp.sum(x * x, axis=1, keepdims=True)) * (0.5 / half)
    r = jnp.broadcast_to(lax.rsqrt(power + NORM_EPS), scale.shape)
    scale[...] = r
    left = (x * gain[:, pl.ds(at, half)]).astype(BF16)
    full[:, pl.ds(at, half)] = left
    full[:, pl.ds(pl.multiple_of(tp[0] * half, half), half)] = xg[...]

    def project(i, lo, hi):
        copies[i].wait()
        s = acc[:, lo:hi] + dot(left, buf[:, lo:hi])
        return (s * tile_lanes(r, hi - lo)).astype(BF16)

    kw = weights[0].shape[1]
    vw = weights[2].shape[1]
    cw = weights[3].shape[1]
    k = project(0, 0, kw)
    key[...] = k
    f = project(1, kw, 2 * kw).astype(F32) + bias[...]
    log = (jnp.minimum(f, 0.0) - jnp.log1p(jnp.exp(-jnp.abs(f)))) * (1.0 / GATE_SOFTNESS)
    log = log + wide[...]
    hi = log.astype(BF16)
    rest = log - hi.astype(F32)
    mid = rest.astype(BF16)
    low = (rest - mid.astype(F32)).astype(BF16)
    tri = (
        lax.broadcasted_iota(jnp.int32, (BLOCK, 3 * BLOCK), 0)
        >= lax.broadcasted_iota(jnp.int32, (BLOCK, 3 * BLOCK), 1) % BLOCK
    ).astype(BF16)
    n = rows // BLOCK
    running = jnp.zeros((1, kw), F32)
    starts = []
    for b in range(n):
        s = slice(b * BLOCK, (b + 1) * BLOCK)
        part = dot(tri, jnp.concatenate([hi[s], mid[s], low[s]], axis=0))
        cum[s, :] = part
        starts.append(running)
        running = running + part[BLOCK - 1 :]
    base[...] = jnp.concatenate(starts + [running] * (base.shape[0] - n), axis=0)
    kf = k.astype(F32)
    decayed = []
    for b in range(n):
        s = slice(b * BLOCK, (b + 1) * BLOCK)
        decayed.append((kf[s] * jnp.exp((running - starts[b]) - cum[s, :])).astype(BF16))
    decayed = jnp.concatenate(decayed, axis=0)
    val[...] = project(2, 2 * kw, 2 * kw + vw)
    dv = own.shape[0]
    group = vw // 256
    for g in range(group):
        m = lax.dot_general(
            val[:, g * 256 : (g + 1) * 256],
            decayed[:, g * 128 : (g + 1) * 128],
            TN,
            preferred_element_type=F32,
        )
        own[:, g * 128 : (g + 1) * 128] = fold(m, dv)
    at = 2 * kw + vw
    c_in = project(3, at, at + cw).astype(F32)
    h_in = project(4, at + cw, at + 2 * cw).astype(F32)
    p = c_in * h_in
    p = p.astype(BF16)
    prod[...] = p
    last = p[rows - 16 :].astype(F32)
    pack(send, own[...], jnp.exp(running), [last[14:15, :kw], last[14:15, kw:], last[15:, :kw], last[15:, kw:]])


def fold(m, dv):
    step = m.shape[1] // (m.shape[0] // dv)
    lane = lax.broadcasted_iota(jnp.int32, (dv, m.shape[1]), 1) // step
    out = m[:dv]
    for h in range(1, m.shape[0] // dv):
        out = jnp.where(lane == h, m[h * dv : (h + 1) * dv], out)
    return out


def pack(ref, state, decay, halo):
    dv = state.shape[0]
    ref[:dv, :] = state.astype(BF16)
    top = decay.astype(BF16).astype(F32)
    row = lax.broadcasted_iota(jnp.int32, (EXTRA_ROWS, state.shape[1]), 0)
    tail = jnp.zeros((EXTRA_ROWS, state.shape[1]), F32)
    for i, v in enumerate([top, decay - top] + list(halo)):
        tail = jnp.where(row == i, v, tail)
    ref[dv:, :] = tail.astype(BF16)


def unpack(v, dv):
    tail = v[dv:].astype(F32)
    return v[:dv].astype(F32), tail[0:1] + tail[1:2], tail


def fold_round(digit, low_zero, stack, radix, dv):
    lanes = stack.shape[2]
    pre_s, pre_d = jnp.zeros((dv, lanes), F32), jnp.ones((1, lanes), F32)
    tot_s, tot_d = pre_s, pre_d
    halo = jnp.zeros((EXTRA_ROWS, lanes), F32)
    for j in range(radix):
        s, d, tail = unpack(stack[j ^ digit], dv)
        before = j < digit
        pre_s = jnp.where(before, d * pre_s + s, pre_s)
        pre_d = jnp.where(before, d * pre_d, pre_d)
        halo = jnp.where((j + 1 == digit) & (low_zero > 0), tail, halo)
        tot_s, tot_d = d * tot_s + s, d * tot_d
    return pre_s, pre_d, tot_s, tot_d, tail, halo


def join_round(radix, place, *refs):
    items, (sp, dp, hp), (send, s_out, d_out, h_out), (stack,) = (
        refs[:radix],
        refs[radix : radix + 3],
        refs[radix + 3 : radix + 7],
        refs[radix + 7 :],
    )
    dv = sp.shape[0]
    for i, item in enumerate(items):
        stack[i] = item[...]
    pre_s, pre_d, tot_s, tot_d, tail, halo = fold_round(place[0], place[1], stack, radix, dv)
    s_out[...] = dp[0:1] * pre_s + sp[...]
    d_out[...] = jnp.broadcast_to(dp[0:1] * pre_d, d_out.shape)
    h_out[...] = halo + hp[...]
    pack(send, tot_s, tot_d, [tail[2:3], tail[3:4], tail[4:5], tail[5:6]])


def late_half(full, scale, prod, taps, gain, wq, wb, wg, query, outer, gate, conv):
    r = scale[...]
    x = full[...]

    def project(w):
        s = dot(x, w[...])
        return (s * tile_lanes(r, s.shape[1])).astype(BF16)

    b = project(wb)
    outer[...] = b
    p = prod[...].astype(F32)
    rows = p.shape[0]
    row = lax.broadcasted_iota(jnp.int32, p.shape, 0)
    t = taps[...].astype(F32)
    total = jnp.zeros(p.shape, F32)
    for j in range(taps.shape[0] - 1):
        back = taps.shape[0] - 1 - j
        total = total + t[j : j + 1] * jnp.where(row >= back, pltpu.roll(p, back, 0), 0.0)
    total = total + t[taps.shape[0] - 1 :] * p
    conv[...] = (b.astype(F32) * total).astype(BF16)
    query[...] = project(wq)
    g = project(wg).astype(F32)
    gate[...] = g * jax.nn.sigmoid(g) * gain[...]


def blockwise(key_dim, query, key, val, cum, base, start, raw, through, first):
    rows = query.shape[0]
    n = rows // BLOCK
    scale = key_dim**-0.5
    first[...] = start[...].T
    k_mask = block_mask(256, 64, 128, 32)
    v_mask = block_mask(256, 64, 256, 64)
    causal = lax.broadcasted_iota(jnp.int32, (BLOCK, 256), 0) >= (
        lax.broadcasted_iota(jnp.int32, (BLOCK, 256), 1) % BLOCK
    )
    zero = jnp.zeros((), BF16)
    for g in range(val.shape[1] // 256):
        kl = slice(g * 128, (g + 1) * 128)
        vl = slice(g * 256, (g + 1) * 256)
        state = None
        for b in range(n):
            s = slice(b * BLOCK, (b + 1) * BLOCK)
            c = cum[s, kl]
            q = query[s, kl].astype(F32) * scale
            k = key[s, kl].astype(F32)
            end = c[BLOCK - 1 :]
            q_in = (q * jnp.exp(c)).astype(BF16)
            k_in = (k * jnp.exp(-c)).astype(BF16)
            through[s, kl] = (q * jnp.exp(c + base[b : b + 1, kl])).astype(BF16)
            v = val[s, vl]
            k_wide = jnp.where(k_mask, jnp.concatenate([k_in] * 4, axis=0), zero)
            scores = lax.dot_general(q_in, k_wide, NT, preferred_element_type=F32)
            scores = jnp.where(causal, scores, 0.0).astype(BF16)
            v_wide = jnp.where(v_mask, jnp.concatenate([v] * 4, axis=0), zero)
            out = dot(scores, v_wide)
            if state is not None:
                out = out + lax.dot_general(
                    q_in, state.astype(BF16), NT, preferred_element_type=F32
                )
            raw[s, vl] = out
            if b < n - 1:
                k_out = (k * jnp.exp(end - c)).astype(BF16)
                new = lax.dot_general(v, k_out, TN, preferred_element_type=F32)
                new = jnp.where(k_mask, new, 0.0)
                state = new if state is None else state * jnp.exp(end) + new


def rows_out(half, incoming, halo, raw, through, gate, conv, outer, prod, taps, wc, wa):
    rows = raw.shape[0] // 2
    at = pl.multiple_of(half * rows, 64)
    here = pl.ds(at, rows)
    ones = block_mask(256, 64, 256, 64).astype(BF16) * (1.0 / 64)
    ones = ones.astype(BF16)
    parts = []
    for g in range(raw.shape[1] // 256):
        vl = slice(g * 256, (g + 1) * 256)
        x = raw[here, vl] + lax.dot_general(
            through[here, g * 128 : (g + 1) * 128],
            incoming[g],
            NT,
            preferred_element_type=F32,
        )
        mean = dot((x * x).astype(BF16), ones)
        parts.append((x * lax.rsqrt(mean + NORM_EPS) * gate[here, vl]).astype(BF16))
    attn = jnp.concatenate(parts, axis=1)
    p = prod[:16, :].astype(F32)
    wide = p.shape[1]
    row = lax.broadcasted_iota(jnp.int32, p.shape, 0)
    t = taps[...].astype(F32)
    back2 = jnp.where(row == 0, halo[0:1], jnp.where(row == 1, halo[1:2], pltpu.roll(p, 2, 0)))
    back1 = jnp.where(row == 0, halo[1:2], pltpu.roll(p, 1, 0))
    top = outer[:16, :].astype(F32) * (t[0:1] * back2 + t[1:2] * back1 + t[2:3] * p)
    mine = conv[here, :]
    head = jnp.where(half == 0, top, mine[:16].astype(F32)).astype(BF16)
    left = jnp.concatenate([head, mine[16:]], axis=0)
    return left, attn


def project_out(left, attn, wc, wa, out):
    step = 512
    for n in range(0, out.shape[1], step):
        s = dot(left, wc[:, n : n + step]) + dot(attn, wa[:, n : n + step])
        out[:, n : n + step] = s.astype(out.dtype)


def partner_rows(radix, place, *refs):
    items = refs[:radix]
    sp, dp, hp, first, raw, through, gate, conv, outer, prod, taps, wc, wa = refs[radix : radix + 13]
    out, state, halo_out, stack = refs[radix + 13 :]
    dv = sp.shape[0]
    for i, item in enumerate(items):
        stack[i] = item[...]
    digit, low_zero, half = place[0], place[1], 1 - place[2]
    lanes = stack.shape[2]
    pre_s = first[...]
    halo = hp[...]
    for j in range(radix):
        s, d, tail = unpack(stack[j ^ digit], dv)
        pre_s = jnp.where(j < digit, d * pre_s + s, pre_s)
        halo = jnp.where((j + 1 == digit) & (low_zero > 0), tail, halo)
    pre_s = dp[0:1] * pre_s + sp[...]
    mask = block_mask(256, 64, 128, 32)
    incoming = []
    for g in range(lanes // 128):
        s = pre_s[:, g * 128 : (g + 1) * 128]
        wide = jnp.where(mask, jnp.concatenate([s] * 4, axis=0), 0.0).astype(BF16)
        incoming.append(wide)
        state[g] = wide
    rows2 = jnp.concatenate(
        [jnp.concatenate([halo[2:3], halo[3:4]], axis=1), jnp.concatenate([halo[4:5], halo[5:6]], axis=1)],
        axis=0,
    )
    halo_out[...] = jnp.concatenate([rows2] * 4, axis=0)
    left, attn = rows_out(half, incoming, rows2, raw, through, gate, conv, outer, prod, taps, wc, wa)
    project_out(left, attn, wc, wa, out)


def own_rows(place, state, halo, raw, through, gate, conv, outer, prod, taps, wc, wa, out):
    incoming = [state[g] for g in range(state.shape[0])]
    left, attn = rows_out(
        place[2], incoming, halo[0:2, :], raw, through, gate, conv, outer, prod, taps, wc, wa
    )
    project_out(left, attn, wc, wa, out)


def add_rows(a, b, out):
    out[...] = (a[...] + b[...].astype(F32)).astype(BF16)


def radices(n):
    found = []
    while n > 1:
        r = 4 if n % 4 == 0 else 2
        found.append(r)
        n //= r
    return found


def on_device(
    tokens,
    input_norm_gain,
    outer_gate_weight,
    inner_gate_weight,
    convolution_input_weight,
    convolution_kernel_taps,
    query_weight_matrix,
    key_weight_matrix,
    value_weight_matrix,
    forget_gate_weight,
    attention_gate_weight,
    forget_gate_bias,
    extra_logarithm_decay,
    initial_head_state,
    head_norm_gain,
    convolution_output_weight,
    attention_output_weight,
):
    rows, half = tokens.shape
    heads, dk, dv = initial_head_state.shape
    kw, vw, cw = heads * dk, heads * dv, outer_gate_weight.shape[1]
    model = convolution_output_weight.shape[1]
    n_sp = lax.axis_size("sp")
    tp = lax.axis_index("tp").astype(jnp.int32)
    sp = lax.axis_index("sp").astype(jnp.int32)
    swap = [(0, 1), (1, 0)]
    other = lax.ppermute(tokens, "tp", swap)
    gain = input_norm_gain.reshape(1, -1)
    tp1 = tp.reshape(1)
    early = (
        key_weight_matrix,
        forget_gate_weight,
        value_weight_matrix,
        inner_gate_weight,
        convolution_input_weight,
    )
    width = sum(w.shape[1] for w in early)
    buffers = [pltpu.VMEM((half, width), BF16), pltpu.SemaphoreType.DMA((5,))]
    flops = 2 * rows * half * width
    acc, xg, ssq, wide = call(
        own_half,
        [((rows, width), F32), ((rows, half), BF16), ((rows, 128), F32), ((rows, kw), F32)],
        [(tp1, SMEM), (tokens, VMEM), (gain, VMEM), (extra_logarithm_decay, VMEM)]
        + [(w, HBM) for w in early],
        flops,
        buffers,
        name="own_half",
    )
    full, scale, key, val, cum, base, prod, own, send = call(
        other_half,
        [
            ((rows, 2 * half), BF16),
            ((rows, 128), F32),
            ((rows, kw), BF16),
            ((rows, vw), BF16),
            ((rows, kw), F32),
            ((8, kw), F32),
            ((rows, cw), BF16),
            ((dv, kw), F32),
            ((dv + EXTRA_ROWS, kw), BF16),
        ],
        [(tp1, SMEM), (other, VMEM), (gain, VMEM), (forget_gate_bias.reshape(1, -1), VMEM)]
        + [(a, VMEM) for a in (acc, xg, ssq, wide)]
        + [(w, HBM) for w in early],
        flops,
        buffers,
        name="other_half",
    )
    query, outer, gate, conv = call(
        late_half,
        [((rows, kw), BF16), ((rows, cw), BF16), ((rows, vw), F32), ((rows, cw), BF16)],
        [
            (full, VMEM),
            (scale, VMEM),
            (prod, VMEM),
            (convolution_kernel_taps, VMEM),
            (jnp.tile(head_norm_gain.reshape(1, -1), (1, heads)), VMEM),
            (query_weight_matrix, VMEM),
            (outer_gate_weight, VMEM),
            (attention_gate_weight, VMEM),
        ],
        2 * rows * 2 * half * (kw + vw + cw),
        name="late_half",
    )
    raw, through, first = call(
        functools.partial(blockwise, dk),
        [((rows, vw), F32), ((rows, kw), BF16), ((dv, kw), F32)],
        [
            (a, VMEM)
            for a in (query, key, val, cum, base, initial_head_state.reshape(heads * dk, dv))
        ],
        2 * rows * 2 * half * (kw + vw),
        name="blockwise",
    )
    pre = (
        jnp.zeros((dv, kw), F32),
        jnp.ones((8, kw), F32),
        jnp.zeros((EXTRA_ROWS, kw), F32),
    )
    stride = 1
    plan = radices(n_sp)
    for turn, radix in enumerate(plan):
        items = [send]
        for j in range(1, radix):
            items.append(lax.ppermute(send, "sp", [(i, i ^ (j * stride)) for i in range(n_sp)]))
        digit = (sp // stride) % radix
        low_zero = (sp % stride == 0).astype(jnp.int32)
        place = jnp.stack([digit, low_zero, tp])
        stack = [pltpu.VMEM((radix,) + send.shape, BF16)]
        if turn < len(plan) - 1:
            send, *pre = call(
                functools.partial(join_round, radix),
                [(send.shape, BF16), ((dv, kw), F32), ((8, kw), F32), ((EXTRA_ROWS, kw), F32)],
                [(place, SMEM)] + [(a, VMEM) for a in items] + [(a, VMEM) for a in pre],
                1 << 20,
                stack,
                name="join_round",
            )
        stride *= radix
    tail = [
        (a, VMEM)
        for a in (
            raw,
            through,
            gate,
            conv,
            outer,
            prod,
            convolution_kernel_taps,
            convolution_output_weight,
            attention_output_weight,
        )
    ]
    flops = 2 * (rows // 2) * model * (vw + cw)
    theirs, state, halo = call(
        functools.partial(partner_rows, plan[-1]),
        [((rows // 2, model), BF16), ((kw // 128, 256, 128), BF16), ((8, cw), F32)],
        [(place, SMEM)] + [(a, VMEM) for a in items] + [(a, VMEM) for a in (*pre, first)] + tail,
        flops,
        stack,
        name="partner_rows",
    )
    got = lax.ppermute(theirs, "tp", swap)
    (mine,) = call(
        own_rows,
        [((rows // 2, model), F32)],
        [(place, SMEM), (state, VMEM), (halo, VMEM)] + tail,
        flops,
        name="own_rows",
    )
    return (mine + got.astype(F32)).astype(BF16)


def solution(mesh):
    placed = (
        P("sp", "tp"),
        P(),
        P(None, "tp"),
        P(None, "tp"),
        P(None, "tp"),
        P(None, "tp"),
        P(None, "tp"),
        P(None, "tp"),
        P(None, "tp"),
        P(None, "tp"),
        P(None, "tp"),
        P("tp"),
        P("sp", "tp"),
        P("tp", None, None),
        P(),
        P("tp", None),
        P("tp", None),
    )
    return jax.shard_map(
        on_device, mesh=mesh, in_specs=placed, out_specs=P(("sp", "tp"), None), check_vma=False
    )
```

```python
import functools

import jax
import jax.numpy as jnp
from jax import lax
from jax.experimental import pallas as pl
from jax.experimental.pallas import tpu as pltpu
from jax.sharding import PartitionSpec as P

BLOCK = 64
NORM_EPS = 1e-06
GATE_SOFTNESS = 16.0
F32 = jnp.float32
BF16 = jnp.bfloat16
NT = (((1,), (1,)), ((), ()))
TN = (((0,), (0,)), ((), ()))
VMEM = pl.BlockSpec(memory_space=pltpu.VMEM)
SMEM = pl.BlockSpec(memory_space=pltpu.SMEM)
HBM = pl.BlockSpec(memory_space=pltpu.HBM)
EXTRA_ROWS = 16


def dot(a, b):
    return jnp.dot(a, b, preferred_element_type=F32)


def call(body, outs, ins, flops, scratch=(), limit=12 << 20, name=None):
    specs = [s for _, s in ins]
    return pl.pallas_call(
        body,
        out_shape=[jax.ShapeDtypeStruct(s, d) for s, d in outs],
        in_specs=specs,
        out_specs=[VMEM] * len(outs),
        scratch_shapes=list(scratch),
        compiler_params=pltpu.CompilerParams(vmem_limit_bytes=limit),
        cost_estimate=pl.CostEstimate(flops=flops, bytes_accessed=1 << 20, transcendentals=0),
        name=name,
    )(*[pltpu.with_memory_space_constraint(a, pltpu.HBM) if s is HBM else a for a, s in ins])


def weight_copies(hbm, buf, sems, row, rows):
    copies, at = [], 0
    for i, w in enumerate(hbm):
        cols = w.shape[1]
        copies.append(
            pltpu.make_async_copy(
                w.at[pl.ds(row, rows), :], buf.at[:, at : at + cols], sems.at[i]
            )
        )
        at += cols
    return copies


def tile_lanes(column, lanes):
    return jnp.concatenate([column] * (lanes // column.shape[1]), axis=1)


def block_mask(rows, row_step, lanes, lane_step):
    r = lax.broadcasted_iota(jnp.int32, (rows, lanes), 0) // row_step
    c = lax.broadcasted_iota(jnp.int32, (rows, lanes), 1) // lane_step
    return r == c


def own_half(tp, tok_hbm, gain_hbm, extra_hbm, *refs):
    weights, (acc, xg, ssq, wide, rest) = refs[:5], refs[5:10]
    buf, sems, tok, gain, extra, small = refs[10:]
    half = tok.shape[1]
    at = pl.multiple_of(tp[0] * half, half)
    loads = [
        pltpu.make_async_copy(src, dst, small.at[i])
        for i, (src, dst) in enumerate([(tok_hbm, tok), (gain_hbm, gain), (extra_hbm, extra)])
    ]
    copies = weight_copies(weights, buf, sems.at[0], at, half)
    away = pl.multiple_of((1 - tp[0]) * half, half)
    ahead = weight_copies(weights, rest, sems.at[1], away, half)
    for c in loads + copies + ahead:
        c.start()
    for c in loads:
        c.wait()
    x = tok[...].astype(F32)
    ssq[...] = jnp.broadcast_to(jnp.sum(x * x, axis=1, keepdims=True), ssq.shape)
    xg[...] = (x * gain[:, pl.ds(at, half)]).astype(BF16)
    heads = extra.shape[0]
    lanes = wide.shape[1]
    r = lax.broadcasted_iota(jnp.int32, (heads, lanes), 0)
    c = lax.broadcasted_iota(jnp.int32, (heads, lanes), 1) // (lanes // heads)
    wide[...] = lax.dot_general(
        extra[...],
        (r == c).astype(F32),
        TN,
        precision=lax.Precision.HIGHEST,
        preferred_element_type=F32,
    )
    left = xg[...]
    at = 0
    for c, w in zip(copies, weights):
        cols = w.shape[1]
        c.wait()
        acc[:, at : at + cols] = dot(left, buf[:, at : at + cols])
        at += cols
    for c in ahead:
        c.wait()


def other_half(
    tp, tok, gain, bias, acc, xg, ssq, wide, wnext,
    full, scale, key, val, cum, base, prod, own, send,
):
    rows, half = tok.shape
    at = pl.multiple_of((1 - tp[0]) * half, half)
    x = tok[...].astype(F32)
    power = (ssq[:, :1] + jnp.sum(x * x, axis=1, keepdims=True)) * (0.5 / half)
    r = jnp.broadcast_to(lax.rsqrt(power + NORM_EPS), scale.shape)
    scale[...] = r
    left = (x * gain[:, pl.ds(at, half)]).astype(BF16)
    full[:, pl.ds(at, half)] = left
    full[:, pl.ds(pl.multiple_of(tp[0] * half, half), half)] = xg[...]

    def project(lo, hi):
        s = acc[:, lo:hi] + dot(left, wnext[:, lo:hi])
        return (s * tile_lanes(r, hi - lo)).astype(BF16)

    kw, vw, cw = key.shape[1], val.shape[1], prod.shape[1]
    k = project(0, kw)
    key[...] = k
    f = project(kw, 2 * kw).astype(F32) + bias[...]
    log = (jnp.minimum(f, 0.0) - jnp.log1p(jnp.exp(-jnp.abs(f)))) * (1.0 / GATE_SOFTNESS)
    log = log + wide[...]
    hi = log.astype(BF16)
    rest = log - hi.astype(F32)
    mid = rest.astype(BF16)
    low = (rest - mid.astype(F32)).astype(BF16)
    tri = (
        lax.broadcasted_iota(jnp.int32, (BLOCK, 3 * BLOCK), 0)
        >= lax.broadcasted_iota(jnp.int32, (BLOCK, 3 * BLOCK), 1) % BLOCK
    ).astype(BF16)
    n = rows // BLOCK
    running = jnp.zeros((1, kw), F32)
    starts = []
    for b in range(n):
        s = slice(b * BLOCK, (b + 1) * BLOCK)
        part = dot(tri, jnp.concatenate([hi[s], mid[s], low[s]], axis=0))
        cum[s, :] = part
        starts.append(running)
        running = running + part[BLOCK - 1 :]
    base[...] = jnp.concatenate(starts + [running] * (base.shape[0] - n), axis=0)
    kf = k.astype(F32)
    decayed = []
    for b in range(n):
        s = slice(b * BLOCK, (b + 1) * BLOCK)
        decayed.append((kf[s] * jnp.exp((running - starts[b]) - cum[s, :])).astype(BF16))
    decayed = jnp.concatenate(decayed, axis=0)
    val[...] = project(2 * kw, 2 * kw + vw)
    dv = own.shape[0]
    group = vw // 256
    for g in range(group):
        m = lax.dot_general(
            val[:, g * 256 : (g + 1) * 256],
            decayed[:, g * 128 : (g + 1) * 128],
            TN,
            preferred_element_type=F32,
        )
        own[:, g * 128 : (g + 1) * 128] = fold(m, dv)
    lo = 2 * kw + vw
    c_in = project(lo, lo + cw).astype(F32)
    h_in = project(lo + cw, lo + 2 * cw).astype(F32)
    p = c_in * h_in
    p = p.astype(BF16)
    prod[...] = p
    last = p[rows - 16 :].astype(F32)
    pack(send, own[...], jnp.exp(running), [last[14:15, :kw], last[14:15, kw:], last[15:, :kw], last[15:, kw:]])


def fold(m, dv):
    step = m.shape[1] // (m.shape[0] // dv)
    lane = lax.broadcasted_iota(jnp.int32, (dv, m.shape[1]), 1) // step
    out = m[:dv]
    for h in range(1, m.shape[0] // dv):
        out = jnp.where(lane == h, m[h * dv : (h + 1) * dv], out)
    return out


def pack(ref, state, decay, halo):
    dv = state.shape[0]
    ref[:dv, :] = state.astype(BF16)
    top = decay.astype(BF16).astype(F32)
    row = lax.broadcasted_iota(jnp.int32, (EXTRA_ROWS, state.shape[1]), 0)
    tail = jnp.zeros((EXTRA_ROWS, state.shape[1]), F32)
    for i, v in enumerate([top, decay - top] + list(halo)):
        tail = jnp.where(row == i, v, tail)
    ref[dv:, :] = tail.astype(BF16)


def unpack(v, dv):
    tail = v[dv:].astype(F32)
    return v[:dv].astype(F32), tail[0:1] + tail[1:2], tail


def fold_round(digit, low_zero, stack, radix, dv):
    lanes = stack.shape[2]
    pre_s, pre_d = jnp.zeros((dv, lanes), F32), jnp.ones((1, lanes), F32)
    tot_s, tot_d = pre_s, pre_d
    halo = jnp.zeros((EXTRA_ROWS, lanes), F32)
    for j in range(radix):
        s, d, tail = unpack(stack[j ^ digit], dv)
        before = j < digit
        pre_s = jnp.where(before, d * pre_s + s, pre_s)
        pre_d = jnp.where(before, d * pre_d, pre_d)
        halo = jnp.where((j + 1 == digit) & (low_zero > 0), tail, halo)
        tot_s, tot_d = d * tot_s + s, d * tot_d
    return pre_s, pre_d, tot_s, tot_d, tail, halo


def join_round(radix, place, *refs):
    items, (sp, dp, hp), (send, s_out, d_out, h_out), (stack,) = (
        refs[:radix],
        refs[radix : radix + 3],
        refs[radix + 3 : radix + 7],
        refs[radix + 7 :],
    )
    dv = sp.shape[0]
    for i, item in enumerate(items):
        stack[i] = item[...]
    pre_s, pre_d, tot_s, tot_d, tail, halo = fold_round(place[0], place[1], stack, radix, dv)
    s_out[...] = dp[0:1] * pre_s + sp[...]
    d_out[...] = jnp.broadcast_to(dp[0:1] * pre_d, d_out.shape)
    h_out[...] = halo + hp[...]
    pack(send, tot_s, tot_d, [tail[2:3], tail[3:4], tail[4:5], tail[5:6]])


def late_half(full, scale, prod, taps, gain, wq, wb, wg, query, outer, gate, conv):
    r = scale[...]
    x = full[...]

    def project(w):
        s = dot(x, w[...])
        return (s * tile_lanes(r, s.shape[1])).astype(BF16)

    b = project(wb)
    outer[...] = b
    p = prod[...].astype(F32)
    rows = p.shape[0]
    row = lax.broadcasted_iota(jnp.int32, p.shape, 0)
    t = taps[...].astype(F32)
    total = jnp.zeros(p.shape, F32)
    for j in range(taps.shape[0] - 1):
        back = taps.shape[0] - 1 - j
        total = total + t[j : j + 1] * jnp.where(row >= back, pltpu.roll(p, back, 0), 0.0)
    total = total + t[taps.shape[0] - 1 :] * p
    conv[...] = (b.astype(F32) * total).astype(BF16)
    query[...] = project(wq)
    g = project(wg).astype(F32)
    gate[...] = g * jax.nn.sigmoid(g) * tile_lanes(gain[...], g.shape[1])


def blockwise(key_dim, query, key, val, cum, base, start, raw, through, first):
    rows = query.shape[0]
    n = rows // BLOCK
    scale = key_dim**-0.5
    first[...] = start[...].T
    k_mask = block_mask(256, 64, 128, 32)
    v_mask = block_mask(256, 64, 256, 64)
    causal = lax.broadcasted_iota(jnp.int32, (BLOCK, 256), 0) >= (
        lax.broadcasted_iota(jnp.int32, (BLOCK, 256), 1) % BLOCK
    )
    zero = jnp.zeros((), BF16)
    for g in range(val.shape[1] // 256):
        kl = slice(g * 128, (g + 1) * 128)
        vl = slice(g * 256, (g + 1) * 256)
        state = None
        for b in range(n):
            s = slice(b * BLOCK, (b + 1) * BLOCK)
            c = cum[s, kl]
            q = query[s, kl].astype(F32) * scale
            k = key[s, kl].astype(F32)
            end = c[BLOCK - 1 :]
            q_in = (q * jnp.exp(c)).astype(BF16)
            k_in = (k * jnp.exp(-c)).astype(BF16)
            through[s, kl] = (q * jnp.exp(c + base[b : b + 1, kl])).astype(BF16)
            v = val[s, vl]
            k_wide = jnp.where(k_mask, jnp.concatenate([k_in] * 4, axis=0), zero)
            scores = lax.dot_general(q_in, k_wide, NT, preferred_element_type=F32)
            scores = jnp.where(causal, scores, 0.0).astype(BF16)
            v_wide = jnp.where(v_mask, jnp.concatenate([v] * 4, axis=0), zero)
            out = dot(scores, v_wide)
            if state is not None:
                out = out + lax.dot_general(
                    q_in, state.astype(BF16), NT, preferred_element_type=F32
                )
            raw[s, vl] = out
            if b < n - 1:
                k_out = (k * jnp.exp(end - c)).astype(BF16)
                new = lax.dot_general(v, k_out, TN, preferred_element_type=F32)
                new = jnp.where(k_mask, new, 0.0)
                state = new if state is None else state * jnp.exp(end) + new


def rows_out(half, incoming, halo, raw, through, gate, conv, outer, prod, taps, wc, wa):
    rows = raw.shape[0] // 2
    at = pl.multiple_of(half * rows, 64)
    here = pl.ds(at, rows)
    ones = block_mask(256, 64, 256, 64).astype(BF16) * (1.0 / 64)
    ones = ones.astype(BF16)
    parts = []
    for g in range(raw.shape[1] // 256):
        vl = slice(g * 256, (g + 1) * 256)
        x = raw[here, vl] + lax.dot_general(
            through[here, g * 128 : (g + 1) * 128],
            incoming[g],
            NT,
            preferred_element_type=F32,
        )
        mean = dot((x * x).astype(BF16), ones)
        parts.append((x * lax.rsqrt(mean + NORM_EPS) * gate[here, vl]).astype(BF16))
    attn = jnp.concatenate(parts, axis=1)
    p = prod[:16, :].astype(F32)
    wide = p.shape[1]
    row = lax.broadcasted_iota(jnp.int32, p.shape, 0)
    t = taps[...].astype(F32)
    back2 = jnp.where(row == 0, halo[0:1], jnp.where(row == 1, halo[1:2], pltpu.roll(p, 2, 0)))
    back1 = jnp.where(row == 0, halo[1:2], pltpu.roll(p, 1, 0))
    top = outer[:16, :].astype(F32) * (t[0:1] * back2 + t[1:2] * back1 + t[2:3] * p)
    mine = conv[here, :]
    head = jnp.where(half == 0, top, mine[:16].astype(F32)).astype(BF16)
    left = jnp.concatenate([head, mine[16:]], axis=0)
    return left, attn


def project_out(left, attn, wc, wa, out):
    step = 512
    for n in range(0, out.shape[1], step):
        s = dot(left, wc[:, n : n + step]) + dot(attn, wa[:, n : n + step])
        out[:, n : n + step] = s.astype(out.dtype)


def partner_rows(radix, place, *refs):
    items = refs[:radix]
    sp, dp, hp, first, raw, through, gate, conv, outer, prod, taps, wc, wa = refs[radix : radix + 13]
    out, state, halo_out, stack = refs[radix + 13 :]
    dv = sp.shape[0]
    for i, item in enumerate(items):
        stack[i] = item[...]
    digit, low_zero, half = place[0], place[1], 1 - place[2]
    lanes = stack.shape[2]
    pre_s = first[...]
    halo = hp[...]
    for j in range(radix):
        s, d, tail = unpack(stack[j ^ digit], dv)
        pre_s = jnp.where(j < digit, d * pre_s + s, pre_s)
        halo = jnp.where((j + 1 == digit) & (low_zero > 0), tail, halo)
    pre_s = dp[0:1] * pre_s + sp[...]
    mask = block_mask(256, 64, 128, 32)
    incoming = []
    for g in range(lanes // 128):
        s = pre_s[:, g * 128 : (g + 1) * 128]
        wide = jnp.where(mask, jnp.concatenate([s] * 4, axis=0), 0.0).astype(BF16)
        incoming.append(wide)
        state[g] = wide
    rows2 = jnp.concatenate(
        [jnp.concatenate([halo[2:3], halo[3:4]], axis=1), jnp.concatenate([halo[4:5], halo[5:6]], axis=1)],
        axis=0,
    )
    halo_out[...] = jnp.concatenate([rows2] * 4, axis=0)
    left, attn = rows_out(half, incoming, rows2, raw, through, gate, conv, outer, prod, taps, wc, wa)
    project_out(left, attn, wc, wa, out)


def own_rows(place, state, halo, raw, through, gate, conv, outer, prod, taps, wc, wa, out):
    incoming = [state[g] for g in range(state.shape[0])]
    left, attn = rows_out(
        place[2], incoming, halo[0:2, :], raw, through, gate, conv, outer, prod, taps, wc, wa
    )
    project_out(left, attn, wc, wa, out)


def add_rows(a, b, out):
    out[...] = (a[...] + b[...].astype(F32)).astype(BF16)


def radices(n):
    found = []
    while n > 1:
        r = 4 if n % 4 == 0 else 2
        found.append(r)
        n //= r
    return found


def on_device(
    tokens,
    input_norm_gain,
    outer_gate_weight,
    inner_gate_weight,
    convolution_input_weight,
    convolution_kernel_taps,
    query_weight_matrix,
    key_weight_matrix,
    value_weight_matrix,
    forget_gate_weight,
    attention_gate_weight,
    forget_gate_bias,
    extra_logarithm_decay,
    initial_head_state,
    head_norm_gain,
    convolution_output_weight,
    attention_output_weight,
):
    rows, half = tokens.shape
    heads, dk, dv = initial_head_state.shape
    kw, vw, cw = heads * dk, heads * dv, outer_gate_weight.shape[1]
    model = convolution_output_weight.shape[1]
    n_sp = lax.axis_size("sp")
    tp = lax.axis_index("tp").astype(jnp.int32)
    sp = lax.axis_index("sp").astype(jnp.int32)
    swap = [(0, 1), (1, 0)]
    other = lax.ppermute(tokens, "tp", swap)
    gain = input_norm_gain.reshape(1, -1)
    tp1 = tp.reshape(1)
    early = (
        key_weight_matrix,
        forget_gate_weight,
        value_weight_matrix,
        inner_gate_weight,
        convolution_input_weight,
    )
    width = sum(w.shape[1] for w in early)
    extra = extra_logarithm_decay.T
    buffers = [
        pltpu.VMEM((half, width), BF16),
        pltpu.SemaphoreType.DMA((2, 5)),
        pltpu.VMEM(tokens.shape, BF16),
        pltpu.VMEM(gain.shape, F32),
        pltpu.VMEM(extra.shape, F32),
        pltpu.SemaphoreType.DMA((3,)),
    ]
    flops = 2 * rows * half * width
    acc, xg, ssq, wide, rest = call(
        own_half,
        [
            ((rows, width), F32),
            ((rows, half), BF16),
            ((rows, 128), F32),
            ((rows, kw), F32),
            ((half, width), BF16),
        ],
        [(tp1, SMEM), (tokens, HBM), (gain, HBM), (extra, HBM)] + [(w, HBM) for w in early],
        flops,
        buffers,
        name="own_half",
    )
    full, scale, key, val, cum, base, prod, own, send = call(
        other_half,
        [
            ((rows, 2 * half), BF16),
            ((rows, 128), F32),
            ((rows, kw), BF16),
            ((rows, vw), BF16),
            ((rows, kw), F32),
            ((8, kw), F32),
            ((rows, cw), BF16),
            ((dv, kw), F32),
            ((dv + EXTRA_ROWS, kw), BF16),
        ],
        [(tp1, SMEM), (other, VMEM), (gain, VMEM), (forget_gate_bias.reshape(1, -1), VMEM)]
        + [(a, VMEM) for a in (acc, xg, ssq, wide, rest)],
        flops,
        name="other_half",
    )
    query, outer, gate, conv = call(
        late_half,
        [((rows, kw), BF16), ((rows, cw), BF16), ((rows, vw), F32), ((rows, cw), BF16)],
        [
            (full, VMEM),
            (scale, VMEM),
            (prod, VMEM),
            (convolution_kernel_taps, VMEM),
            (head_norm_gain.reshape(1, -1), VMEM),
            (query_weight_matrix, VMEM),
            (outer_gate_weight, VMEM),
            (attention_gate_weight, VMEM),
        ],
        2 * rows * 2 * half * (kw + vw + cw),
        name="late_half",
    )
    raw, through, first = call(
        functools.partial(blockwise, dk),
        [((rows, vw), F32), ((rows, kw), BF16), ((dv, kw), F32)],
        [
            (a, VMEM)
            for a in (query, key, val, cum, base, initial_head_state.reshape(heads * dk, dv))
        ],
        2 * rows * 2 * half * (kw + vw),
        name="blockwise",
    )
    pre = (
        jnp.zeros((dv, kw), F32),
        jnp.ones((8, kw), F32),
        jnp.zeros((EXTRA_ROWS, kw), F32),
    )
    stride = 1
    plan = radices(n_sp)
    for turn, radix in enumerate(plan):
        items = [send]
        for j in range(1, radix):
            items.append(lax.ppermute(send, "sp", [(i, i ^ (j * stride)) for i in range(n_sp)]))
        digit = (sp // stride) % radix
        low_zero = (sp % stride == 0).astype(jnp.int32)
        place = jnp.stack([digit, low_zero, tp])
        stack = [pltpu.VMEM((radix,) + send.shape, BF16)]
        if turn < len(plan) - 1:
            send, *pre = call(
                functools.partial(join_round, radix),
                [(send.shape, BF16), ((dv, kw), F32), ((8, kw), F32), ((EXTRA_ROWS, kw), F32)],
                [(place, SMEM)] + [(a, VMEM) for a in items] + [(a, VMEM) for a in pre],
                1 << 20,
                stack,
                name="join_round",
            )
        stride *= radix
    tail = [
        (a, VMEM)
        for a in (
            raw,
            through,
            gate,
            conv,
            outer,
            prod,
            convolution_kernel_taps,
            convolution_output_weight,
            attention_output_weight,
        )
    ]
    flops = 2 * (rows // 2) * model * (vw + cw)
    theirs, state, halo = call(
        functools.partial(partner_rows, plan[-1]),
        [((rows // 2, model), BF16), ((kw // 128, 256, 128), BF16), ((8, cw), F32)],
        [(place, SMEM)] + [(a, VMEM) for a in items] + [(a, VMEM) for a in (*pre, first)] + tail,
        flops,
        stack,
        name="partner_rows",
    )
    got = lax.ppermute(theirs, "tp", swap)
    (mine,) = call(
        own_rows,
        [((rows // 2, model), F32)],
        [(place, SMEM), (state, VMEM), (halo, VMEM)] + tail,
        flops,
        name="own_rows",
    )
    return (mine + got.astype(F32)).astype(BF16)


def solution(mesh):
    placed = (
        P("sp", "tp"),
        P(),
        P(None, "tp"),
        P(None, "tp"),
        P(None, "tp"),
        P(None, "tp"),
        P(None, "tp"),
        P(None, "tp"),
        P(None, "tp"),
        P(None, "tp"),
        P(None, "tp"),
        P("tp"),
        P("sp", "tp"),
        P("tp", None, None),
        P(),
        P("tp", None),
        P("tp", None),
    )
    return jax.shard_map(
        on_device, mesh=mesh, in_specs=placed, out_specs=P(("sp", "tp"), None), check_vma=False
    )
```

```python
import functools

import jax
import jax.numpy as jnp
from jax import lax
from jax.experimental import pallas as pl
from jax.experimental.pallas import tpu as pltpu
from jax.sharding import PartitionSpec as P


BLOCK = 64
NORM_EPS = 1e-06
GATE_SOFTNESS = 16.0
F32 = jnp.float32
BF16 = jnp.bfloat16
NT = (((1,), (1,)), ((), ()))
TN = (((0,), (0,)), ((), ()))
VMEM = pl.BlockSpec(memory_space=pltpu.VMEM)
HBM = pl.BlockSpec(memory_space=pltpu.HBM)
EXTRA_ROWS = 16


def dot(a, b):
    return jnp.dot(a, b, preferred_element_type=F32)


def call(body, outs, ins, flops, scratch=(), limit=12 << 20):
    specs = [s for _, s in ins]
    return pl.pallas_call(
        body,
        out_shape=[jax.ShapeDtypeStruct(s, d) for s, d in outs],
        in_specs=specs,
        out_specs=[VMEM] * len(outs),
        scratch_shapes=list(scratch),
        compiler_params=pltpu.CompilerParams(vmem_limit_bytes=limit),
        cost_estimate=pl.CostEstimate(flops=flops, bytes_accessed=1 << 20, transcendentals=0),
    )(*[pltpu.with_memory_space_constraint(a, pltpu.HBM) if s is HBM else a for a, s in ins])


def weight_copies(hbm, buf, sems, row, rows):
    copies, at = [], 0
    for i, w in enumerate(hbm):
        cols = w.shape[1]
        copies.append(
            pltpu.make_async_copy(
                w.at[pl.ds(row, rows), :], buf.at[:, at : at + cols], sems.at[i]
            )
        )
        at += cols
    return copies


def tile_lanes(column, lanes):
    return jnp.concatenate([column] * (lanes // column.shape[1]), axis=1)


def block_mask(rows, row_step, lanes, lane_step):
    r = lax.broadcasted_iota(jnp.int32, (rows, lanes), 0) // row_step
    c = lax.broadcasted_iota(jnp.int32, (rows, lanes), 1) // lane_step
    return r == c


def own_half(tok_hbm, gain_hbm, extra_hbm, *refs):
    n = len(refs) - 11
    weights, (acc, xg, ssq, wide, ahead) = refs[:n], refs[n : n + 5]
    buf, sems, tok, gain, extra, small = refs[n + 5 :]
    tp = lax.axis_index("tp")
    half = tok.shape[1]
    here = pl.multiple_of(tp * half, half)
    away = pl.multiple_of((1 - tp) * half, half)
    loads = [
        pltpu.make_async_copy(src, dst, small.at[i])
        for i, (src, dst) in enumerate([(extra_hbm, extra), (gain_hbm, gain), (tok_hbm, tok)])
    ]
    copies = weight_copies(weights, buf, sems.at[0], here, half)
    more = weight_copies(weights, ahead, sems.at[1], away, half)
    for c in loads + copies:
        c.start()
    loads[0].wait()
    heads = extra.shape[0]
    lanes = wide.shape[1]
    r = lax.broadcasted_iota(jnp.int32, (heads, lanes), 0)
    c = lax.broadcasted_iota(jnp.int32, (heads, lanes), 1) // (lanes // heads)
    wide[...] = lax.dot_general(
        extra[...],
        (r == c).astype(F32),
        TN,
        precision=lax.Precision.HIGHEST,
        preferred_element_type=F32,
    )
    loads[1].wait()
    loads[2].wait()
    for c in more:
        c.start()
    x = tok[...].astype(F32)
    ssq[...] = jnp.broadcast_to(jnp.sum(x * x, axis=1, keepdims=True), ssq.shape)
    left = (x * gain[:, pl.ds(here, half)]).astype(BF16)
    xg[...] = left
    for c in copies:
        c.wait()
    acc[...] = dot(left, buf[...])
    for c in more:
        c.wait()


def other_half(
    tok, gain, bias, acc, xg, ssq, wide, wnext, full, scale, key, val, cum, base, send
):
    tp = lax.axis_index("tp")
    rows, half = tok.shape
    here = pl.multiple_of(tp * half, half)
    away = pl.multiple_of((1 - tp) * half, half)
    x = tok[...].astype(F32)
    power = (ssq[:, :1] + jnp.sum(x * x, axis=1, keepdims=True)) * (0.5 / half)
    r = jnp.broadcast_to(lax.rsqrt(power + NORM_EPS), scale.shape)
    scale[...] = r
    left = (x * gain[:, pl.ds(away, half)]).astype(BF16)
    full[:, pl.ds(away, half)] = left
    full[:, pl.ds(here, half)] = xg[...]

    def project(lo, hi):
        s = acc[:, lo:hi] + dot(left, wnext[:, lo:hi])
        return (s * tile_lanes(r, hi - lo)).astype(BF16)

    kw, vw = key.shape[1], val.shape[1]
    k = project(0, kw)
    key[...] = k
    f = project(kw, 2 * kw).astype(F32) + bias[...]
    log = (jnp.minimum(f, 0.0) - jnp.log1p(jnp.exp(-jnp.abs(f)))) * (1.0 / GATE_SOFTNESS)
    log = log + wide[...]
    hi = log.astype(BF16)
    rest = log - hi.astype(F32)
    mid = rest.astype(BF16)
    low = (rest - mid.astype(F32)).astype(BF16)
    tri = (
        lax.broadcasted_iota(jnp.int32, (BLOCK, 3 * BLOCK), 0)
        >= lax.broadcasted_iota(jnp.int32, (BLOCK, 3 * BLOCK), 1) % BLOCK
    ).astype(BF16)
    n = rows // BLOCK
    running = jnp.zeros((1, kw), F32)
    starts, parts = [], []
    for b in range(n):
        s = slice(b * BLOCK, (b + 1) * BLOCK)
        part = dot(tri, jnp.concatenate([hi[s], mid[s], low[s]], axis=0))
        cum[s, :] = part
        parts.append(part)
        starts.append(running)
        running = running + part[BLOCK - 1 :]
    base[...] = jnp.concatenate(starts + [running] * (base.shape[0] - n), axis=0)
    kf = k.astype(F32)
    decayed = []
    for b in range(n):
        s = slice(b * BLOCK, (b + 1) * BLOCK)
        decayed.append((kf[s] * jnp.exp((running - starts[b]) - parts[b])).astype(BF16))
    decayed = jnp.concatenate(decayed, axis=0)
    v = project(2 * kw, 2 * kw + vw)
    val[...] = v
    dv = send.shape[0] - EXTRA_ROWS
    states = []
    for g in range(vw // 256):
        m = lax.dot_general(
            v[:, g * 256 : (g + 1) * 256],
            decayed[:, g * 128 : (g + 1) * 128],
            TN,
            preferred_element_type=F32,
        )
        states.append(fold(m, dv))
    pack(send, jnp.concatenate(states, axis=1), jnp.exp(running))


def fold(m, dv):
    step = m.shape[1] // (m.shape[0] // dv)
    lane = lax.broadcasted_iota(jnp.int32, (dv, m.shape[1]), 1) // step
    out = m[:dv]
    for h in range(1, m.shape[0] // dv):
        out = jnp.where(lane == h, m[h * dv : (h + 1) * dv], out)
    return out


def pack(ref, state, decay, halo=None):
    dv = state.shape[0]
    ref[:dv, :] = state.astype(BF16)
    top = decay.astype(BF16).astype(F32)
    row = lax.broadcasted_iota(jnp.int32, (EXTRA_ROWS, state.shape[1]), 0)
    tail = jnp.where(row == 0, top, decay - top)
    if halo is not None:
        tail = jnp.where(row < 2, tail, halo)
    ref[dv:, :] = tail.astype(BF16)


def unpack(v, dv):
    tail = v[dv:].astype(F32)
    return v[:dv].astype(F32), tail[0:1] + tail[1:2], tail


def to_tail(last):
    width = last.shape[1] // 2
    row = lax.broadcasted_iota(jnp.int32, (EXTRA_ROWS, width), 0)
    tail = jnp.zeros((EXTRA_ROWS, width), F32)
    end = last.shape[0]
    for i in range(4):
        at = end - 2 + i // 2
        part = last[at : at + 1, (i % 2) * width : (i % 2 + 1) * width]
        tail = jnp.where(row == 2 + i, part, tail)
    return tail


def from_tail(tail):
    return jnp.concatenate(
        [
            jnp.concatenate([tail[2:3], tail[3:4]], axis=1),
            jnp.concatenate([tail[4:5], tail[5:6]], axis=1),
        ],
        axis=0,
    )


def fill(stack, items):
    for i, item in enumerate(items):
        stack[i] = item[...]


def halo_of_round(halo, stack, radix, stride, digit, dv):
    low_zero = lax.rem(lax.axis_index("sp"), stride) == 0
    for j in range(radix - 1):
        tail = stack[j ^ digit][dv:].astype(F32)
        halo = jnp.where((j + 1 == digit) & low_zero, tail, halo)
    return halo


def join_round(radix, stride, *refs):
    items, (sp, dp, cross, hp), (send, s_out, d_out, h_out), (stack,) = (
        refs[:radix],
        refs[radix : radix + 4],
        refs[radix + 4 : radix + 8],
        refs[radix + 8 :],
    )
    dv = sp.shape[0]
    fill(stack, items)
    digit = lax.rem(lax.axis_index("sp") // stride, radix)
    lanes = stack.shape[2]
    pre_s, pre_d = jnp.zeros((dv, lanes), F32), jnp.ones((1, lanes), F32)
    tot_s, tot_d = pre_s, pre_d
    for j in range(radix):
        s, d, tail = unpack(stack[j ^ digit], dv)
        before = j < digit
        pre_s = jnp.where(before, d * pre_s + s, pre_s)
        pre_d = jnp.where(before, d * pre_d, pre_d)
        tot_s, tot_d = d * tot_s + s, d * tot_d
    s_out[...] = dp[0:1] * pre_s + sp[...]
    d_out[...] = jnp.broadcast_to(dp[0:1] * pre_d, d_out.shape)
    if stride == 1:
        tail = to_tail(cross[...].astype(F32))
        h_out[...] = jnp.where(digit == 0, 0.0, tail)
    else:
        h_out[...] = halo_of_round(hp[...], stack, radix, stride, digit, dv)
    pack(send, tot_s, tot_d, tail)


def scaled(x, w, r):
    s = dot(x, w)
    return (s * tile_lanes(r, s.shape[1])).astype(BF16)


def conv_inputs(full, scale, wc, wh, prod, last):
    r = scale[...]
    x = full[...]
    p = scaled(x, wc[...], r).astype(F32) * scaled(x, wh[...], r).astype(F32)
    p = p.astype(BF16)
    prod[...] = p
    last[...] = p[p.shape[0] - last.shape[0] :]


def late_half(full, scale, taps, wb, wq, prod, query, outer, conv):
    r = scale[...]
    x = full[...]
    b = scaled(x, wb[...], r)
    outer[...] = b
    p = prod[...].astype(F32)
    row = lax.broadcasted_iota(jnp.int32, p.shape, 0)
    t = taps[...].astype(F32)
    total = jnp.zeros(p.shape, F32)
    for j in range(taps.shape[0] - 1):
        back = taps.shape[0] - 1 - j
        total = total + t[j : j + 1] * jnp.where(row >= back, pltpu.roll(p, back, 0), 0.0)
    total = total + t[taps.shape[0] - 1 :] * p
    conv[...] = (b.astype(F32) * total).astype(BF16)
    query[...] = scaled(x, wq[...], r)


def blockwise(
    key_dim, query, key, val, cum, base, start, full, scale, wg, gain, raw, through, first, gate
):
    rows = query.shape[0]
    n = rows // BLOCK
    shrink = key_dim**-0.5
    first[...] = start[...].T
    gated = scaled(full[...], wg[...], scale[...]).astype(F32)
    gate[...] = gated * jax.nn.sigmoid(gated) * tile_lanes(gain[...], gated.shape[1])
    k_mask = block_mask(256, 64, 128, 32)
    v_mask = block_mask(256, 64, 256, 64)
    causal = lax.broadcasted_iota(jnp.int32, (BLOCK, 256), 0) >= (
        lax.broadcasted_iota(jnp.int32, (BLOCK, 256), 1) % BLOCK
    )
    zero = jnp.zeros((), BF16)
    for g in range(val.shape[1] // 256):
        kl = slice(g * 128, (g + 1) * 128)
        vl = slice(g * 256, (g + 1) * 256)
        state = None
        for b in range(n):
            s = slice(b * BLOCK, (b + 1) * BLOCK)
            c = cum[s, kl]
            q = query[s, kl].astype(F32) * shrink
            k = key[s, kl].astype(F32)
            end = c[BLOCK - 1 :]
            q_in = (q * jnp.exp(c)).astype(BF16)
            k_in = (k * jnp.exp(-c)).astype(BF16)
            through[s, kl] = (q * jnp.exp(c + base[b : b + 1, kl])).astype(BF16)
            v = val[s, vl]
            k_wide = jnp.where(k_mask, jnp.concatenate([k_in] * 4, axis=0), zero)
            scores = lax.dot_general(q_in, k_wide, NT, preferred_element_type=F32)
            scores = jnp.where(causal, scores, 0.0).astype(BF16)
            v_wide = jnp.where(v_mask, jnp.concatenate([v] * 4, axis=0), zero)
            out = dot(scores, v_wide)
            if state is not None:
                out = out + lax.dot_general(
                    q_in, state.astype(BF16), NT, preferred_element_type=F32
                )
            raw[s, vl] = out
            if b < n - 1:
                k_out = (k * jnp.exp(end - c)).astype(BF16)
                new = lax.dot_general(v, k_out, TN, preferred_element_type=F32)
                new = jnp.where(k_mask, new, 0.0)
                state = new if state is None else state * jnp.exp(end) + new


def rows_out(half, incoming, halo, raw, through, gate, conv, outer, prod, taps):
    rows = raw.shape[0] // 2
    at = pl.multiple_of(half * rows, 64)
    here = pl.ds(at, rows)
    ones = block_mask(256, 64, 256, 64).astype(BF16) * (1.0 / 64)
    ones = ones.astype(BF16)
    parts = []
    for g in range(raw.shape[1] // 256):
        vl = slice(g * 256, (g + 1) * 256)
        x = raw[here, vl] + lax.dot_general(
            through[here, g * 128 : (g + 1) * 128],
            incoming[g],
            NT,
            preferred_element_type=F32,
        )
        mean = dot((x * x).astype(BF16), ones)
        parts.append((x * lax.rsqrt(mean + NORM_EPS) * gate[here, vl]).astype(BF16))
    attn = jnp.concatenate(parts, axis=1)
    p = prod[:16, :].astype(F32)
    row = lax.broadcasted_iota(jnp.int32, p.shape, 0)
    t = taps[...].astype(F32)
    back2 = jnp.where(row == 0, halo[0:1], jnp.where(row == 1, halo[1:2], pltpu.roll(p, 2, 0)))
    back1 = jnp.where(row == 0, halo[1:2], pltpu.roll(p, 1, 0))
    top = outer[:16, :].astype(F32) * (t[0:1] * back2 + t[1:2] * back1 + t[2:3] * p)
    mine = conv[here, :]
    head = jnp.where(half == 0, top, mine[:16].astype(F32)).astype(BF16)
    left = jnp.concatenate([head, mine[16:]], axis=0)
    return left, attn


def project_out(left, attn, wc, wa, out):
    step = 512
    for n in range(0, out.shape[1], step):
        s = dot(left, wc[:, n : n + step]) + dot(attn, wa[:, n : n + step])
        out[:, n : n + step] = s.astype(out.dtype)


def partner_rows(radix, stride, *refs):
    items = refs[:radix]
    sp, dp, hp, odd, first, raw, through, gate, conv, outer, prod, taps, wc, wa = refs[
        radix : radix + 14
    ]
    out, state, halo_out, stack = refs[radix + 14 :]
    dv = sp.shape[0]
    fill(stack, items)
    digit = lax.rem(lax.axis_index("sp") // stride, radix)
    lanes = stack.shape[2]
    pre_s = first[...]
    for j in range(radix - 1):
        s, d, _ = unpack(stack[j ^ digit], dv)
        pre_s = jnp.where(j < digit, d * pre_s + s, pre_s)
    pre_s = dp[0:1] * pre_s + sp[...]
    mask = block_mask(256, 64, 128, 32)
    incoming = []
    for g in range(lanes // 128):
        s = pre_s[:, g * 128 : (g + 1) * 128]
        wide = jnp.where(mask, jnp.concatenate([s] * 4, axis=0), 0.0).astype(BF16)
        incoming.append(wide)
        state[g] = wide
    halo = from_tail(halo_of_round(hp[...], stack, radix, stride, digit, dv))
    near = odd[...].astype(F32)[odd.shape[0] - 2 :]
    halo = jnp.where(lax.rem(lax.axis_index("sp"), 2) == 1, near, halo)
    halo_out[...] = jnp.concatenate([halo] * 4, axis=0)
    half = 1 - lax.axis_index("tp")
    left, attn = rows_out(half, incoming, halo, raw, through, gate, conv, outer, prod, taps)
    project_out(left, attn, wc, wa, out)


def own_rows(state, halo, raw, through, gate, conv, outer, prod, taps, wc, wa, out):
    incoming = [state[g] for g in range(state.shape[0])]
    half = lax.axis_index("tp")
    left, attn = rows_out(
        half, incoming, halo[0:2, :], raw, through, gate, conv, outer, prod, taps
    )
    project_out(left, attn, wc, wa, out)


def radices(n):
    found = []
    while n > 1:
        r = 4 if n % 4 == 0 else 2
        found.append(r)
        n //= r
    return found


def on_device(
    tokens,
    input_norm_gain,
    outer_gate_weight,
    inner_gate_weight,
    convolution_input_weight,
    convolution_kernel_taps,
    query_weight_matrix,
    key_weight_matrix,
    value_weight_matrix,
    forget_gate_weight,
    attention_gate_weight,
    forget_gate_bias,
    extra_logarithm_decay,
    initial_head_state,
    head_norm_gain,
    convolution_output_weight,
    attention_output_weight,
):
    rows, half = tokens.shape
    heads, dk, dv = initial_head_state.shape
    kw, vw, cw = heads * dk, heads * dv, outer_gate_weight.shape[1]
    model = convolution_output_weight.shape[1]
    n_sp = lax.axis_size("sp")
    swap = [(0, 1), (1, 0)]
    other = lax.ppermute(tokens, "tp", swap)
    gain = input_norm_gain.reshape(1, -1)
    early = (key_weight_matrix, forget_gate_weight, value_weight_matrix)
    width = sum(w.shape[1] for w in early)
    extra = extra_logarithm_decay.T
    flops = 2 * rows * half * width
    acc, xg, ssq, wide, ahead = call(
        own_half,
        [
            ((rows, width), F32),
            ((rows, half), BF16),
            ((rows, 128), F32),
            ((rows, kw), F32),
            ((half, width), BF16),
        ],
        [(tokens, HBM), (gain, HBM), (extra, HBM)] + [(w, HBM) for w in early],
        flops,
        [
            pltpu.VMEM((half, width), BF16),
            pltpu.SemaphoreType.DMA((2, len(early))),
            pltpu.VMEM(tokens.shape, BF16),
            pltpu.VMEM(gain.shape, F32),
            pltpu.VMEM(extra.shape, F32),
            pltpu.SemaphoreType.DMA((3,)),
        ],
    )
    full, scale, key, val, cum, base, send = call(
        other_half,
        [
            ((rows, 2 * half), BF16),
            ((rows, 128), F32),
            ((rows, kw), BF16),
            ((rows, vw), BF16),
            ((rows, kw), F32),
            ((8, kw), F32),
            ((dv + EXTRA_ROWS, kw), BF16),
        ],
        [(other, VMEM), (gain, VMEM), (forget_gate_bias.reshape(1, -1), VMEM)]
        + [(a, VMEM) for a in (acc, xg, ssq, wide, ahead)],
        flops,
    )
    prod, last = call(
        conv_inputs,
        [((rows, cw), BF16), ((16, cw), BF16)],
        [(a, VMEM) for a in (full, scale, inner_gate_weight, convolution_input_weight)],
        2 * rows * 2 * half * 2 * cw,
    )
    odd = lax.ppermute(last, "sp", [(i, i ^ 1) for i in range(n_sp)])
    cross = lax.ppermute(last, "sp", [(i, i ^ 3) for i in range(n_sp)])
    query, outer, conv = call(
        late_half,
        [((rows, kw), BF16), ((rows, cw), BF16), ((rows, cw), BF16)],
        [
            (a, VMEM)
            for a in (
                full,
                scale,
                convolution_kernel_taps,
                outer_gate_weight,
                query_weight_matrix,
                prod,
            )
        ],
        2 * rows * 2 * half * (kw + cw),
    )
    raw, through, first, gate = call(
        functools.partial(blockwise, dk),
        [((rows, vw), F32), ((rows, kw), BF16), ((dv, kw), F32), ((rows, vw), F32)],
        [
            (a, VMEM)
            for a in (
                query,
                key,
                val,
                cum,
                base,
                initial_head_state.reshape(heads * dk, dv),
                full,
                scale,
                attention_gate_weight,
                head_norm_gain.reshape(1, -1),
            )
        ],
        2 * rows * 2 * half * (kw + vw),
    )
    pre = (jnp.zeros((dv, kw), F32), jnp.ones((8, kw), F32))
    halo = jnp.zeros((EXTRA_ROWS, kw), F32)
    stride = 1
    plan = radices(n_sp)
    for turn, radix in enumerate(plan):
        items = [send]
        for j in range(1, radix):
            pairs = [(i, i ^ (j * stride)) for i in range(n_sp)]
            items.append(lax.ppermute(send, "sp", pairs))
        stack = [pltpu.VMEM((radix,) + send.shape, BF16)]
        if turn < len(plan) - 1:
            send, *pre, halo = call(
                functools.partial(join_round, radix, stride),
                [
                    (send.shape, BF16),
                    ((dv, kw), F32),
                    ((8, kw), F32),
                    ((EXTRA_ROWS, kw), F32),
                ],
                [(a, VMEM) for a in (*items, *pre, cross, halo)],
                1 << 20,
                stack,
            )
            stride *= radix
    tail = [
        (a, VMEM)
        for a in (
            raw,
            through,
            gate,
            conv,
            outer,
            prod,
            convolution_kernel_taps,
            convolution_output_weight,
            attention_output_weight,
        )
    ]
    flops = 2 * (rows // 2) * model * (vw + cw)
    theirs, state, halo = call(
        functools.partial(partner_rows, plan[-1], stride),
        [((rows // 2, model), BF16), ((kw // 128, 256, 128), BF16), ((8, cw), F32)],
        [(a, VMEM) for a in (*items, *pre, halo, odd, first)] + tail,
        flops,
        stack,
    )
    got = lax.ppermute(theirs, "tp", swap)
    (mine,) = call(
        own_rows,
        [((rows // 2, model), F32)],
        [(state, VMEM), (halo, VMEM)] + tail,
        flops,
    )
    return (mine + got.astype(F32)).astype(BF16)


def solution(mesh):
    placed = (
        P("sp", "tp"),
        P(),
        P(None, "tp"),
        P(None, "tp"),
        P(None, "tp"),
        P(None, "tp"),
        P(None, "tp"),
        P(None, "tp"),
        P(None, "tp"),
        P(None, "tp"),
        P(None, "tp"),
        P("tp"),
        P("sp", "tp"),
        P("tp", None, None),
        P(),
        P("tp", None),
        P("tp", None),
    )

    return jax.shard_map(
        on_device, mesh=mesh, in_specs=placed, out_specs=P(("sp", "tp"), None), check_vma=False
    )
```

```python
import functools

import jax
import jax.numpy as jnp
from jax import lax
from jax.experimental import pallas as pl
from jax.experimental.pallas import tpu as pltpu
from jax.sharding import PartitionSpec as P


BLOCK = 64
NORM_EPS = 1e-06
GATE_SOFTNESS = 16.0
F32 = jnp.float32
BF16 = jnp.bfloat16
NT = (((1,), (1,)), ((), ()))
TN = (((0,), (0,)), ((), ()))
VMEM = pl.BlockSpec(memory_space=pltpu.VMEM)
HBM = pl.BlockSpec(memory_space=pltpu.HBM)
EXTRA_ROWS = 8
CHUNKS = 4
FIRST = (2, 3, 1)
LAST = (3, 2, 1)


def dot(a, b):
    return jnp.dot(a, b, preferred_element_type=F32)


def call(body, outs, ins, flops, scratch=(), limit=12 << 20):
    specs = [s for _, s in ins]
    return pl.pallas_call(
        body,
        out_shape=[jax.ShapeDtypeStruct(s, d) for s, d in outs],
        in_specs=specs,
        out_specs=[VMEM] * len(outs),
        scratch_shapes=list(scratch),
        compiler_params=pltpu.CompilerParams(vmem_limit_bytes=limit),
        cost_estimate=pl.CostEstimate(flops=flops, bytes_accessed=1 << 20, transcendentals=0),
    )(*[pltpu.with_memory_space_constraint(a, pltpu.HBM) if s is HBM else a for a, s in ins])


def weight_copies(hbm, buf, sems, row, rows):
    copies, at = [], 0
    for i, w in enumerate(hbm):
        cols = w.shape[1]
        copies.append(
            pltpu.make_async_copy(
                w.at[pl.ds(row, rows), :], buf.at[:, at : at + cols], sems.at[i]
            )
        )
        at += cols
    return copies


def tile_lanes(column, lanes):
    return jnp.concatenate([column] * (lanes // column.shape[1]), axis=1)


def block_mask(rows, row_step, lanes, lane_step):
    r = lax.broadcasted_iota(jnp.int32, (rows, lanes), 0) // row_step
    c = lax.broadcasted_iota(jnp.int32, (rows, lanes), 1) // lane_step
    return r == c


def own_half(tok_hbm, gain_hbm, extra_hbm, *refs):
    n = len(refs) - 11
    weights, (acc, xg, ssq, wide, ahead) = refs[:n], refs[n : n + 5]
    buf, sems, tok, gain, extra, small = refs[n + 5 :]
    tp = lax.axis_index("tp")
    half = tok.shape[1]
    here = pl.multiple_of(tp * half, half)
    away = pl.multiple_of((1 - tp) * half, half)
    loads = [
        pltpu.make_async_copy(src, dst, small.at[i])
        for i, (src, dst) in enumerate([(extra_hbm, extra), (gain_hbm, gain), (tok_hbm, tok)])
    ]
    copies = weight_copies(weights, buf, sems.at[0], here, half)
    more = weight_copies(weights, ahead, sems.at[1], away, half)
    for c in loads + copies:
        c.start()
    loads[0].wait()
    loads[1].wait()
    loads[2].wait()
    for c in more:
        c.start()
    for c in copies:
        c.wait()
    heads = extra.shape[0]
    lanes = wide.shape[1]
    r = lax.broadcasted_iota(jnp.int32, (heads, lanes), 0)
    c = lax.broadcasted_iota(jnp.int32, (heads, lanes), 1) // (lanes // heads)
    wide[...] = lax.dot_general(
        extra[...],
        (r == c).astype(F32),
        TN,
        precision=lax.Precision.HIGHEST,
        preferred_element_type=F32,
    )
    x = tok[...].astype(F32)
    ssq[...] = jnp.broadcast_to(jnp.sum(x * x, axis=1, keepdims=True), ssq.shape)
    left = (x * gain[:, pl.ds(here, half)]).astype(BF16)
    xg[...] = left
    acc[...] = dot(left, buf[...])
    for c in more:
        c.wait()


def other_half(
    tok, gain, bias, acc, xg, ssq, wide, wnext, full, scale, key, val, cum, base, send
):
    tp = lax.axis_index("tp")
    rows, half = tok.shape
    here = pl.multiple_of(tp * half, half)
    away = pl.multiple_of((1 - tp) * half, half)
    x = tok[...].astype(F32)
    power = (ssq[:, :1] + jnp.sum(x * x, axis=1, keepdims=True)) * (0.5 / half)
    r = jnp.broadcast_to(lax.rsqrt(power + NORM_EPS), scale.shape)
    scale[...] = r
    left = (x * gain[:, pl.ds(away, half)]).astype(BF16)
    full[:, pl.ds(away, half)] = left
    full[:, pl.ds(here, half)] = xg[...]

    def project(lo, hi):
        s = acc[:, lo:hi] + dot(left, wnext[:, lo:hi])
        return (s * tile_lanes(r, hi - lo)).astype(BF16)

    kw, vw = key.shape[1], val.shape[1]
    k = project(0, kw)
    key[...] = k
    f = project(kw, 2 * kw).astype(F32) + bias[...]
    log = (jnp.minimum(f, 0.0) - jnp.log1p(jnp.exp(-jnp.abs(f)))) * (1.0 / GATE_SOFTNESS)
    log = log + wide[...]
    hi = log.astype(BF16)
    rest = log - hi.astype(F32)
    mid = rest.astype(BF16)
    low = (rest - mid.astype(F32)).astype(BF16)
    tri = (
        lax.broadcasted_iota(jnp.int32, (BLOCK, 3 * BLOCK), 0)
        >= lax.broadcasted_iota(jnp.int32, (BLOCK, 3 * BLOCK), 1) % BLOCK
    ).astype(BF16)
    n = rows // BLOCK
    running = jnp.zeros((1, kw), F32)
    starts, parts = [], []
    for b in range(n):
        s = slice(b * BLOCK, (b + 1) * BLOCK)
        part = dot(tri, jnp.concatenate([hi[s], mid[s], low[s]], axis=0))
        cum[s, :] = part
        parts.append(part)
        starts.append(running)
        running = running + part[BLOCK - 1 :]
    base[...] = jnp.concatenate(starts + [running] * (base.shape[0] - n), axis=0)
    kf = k.astype(F32)
    decayed = []
    for b in range(n):
        s = slice(b * BLOCK, (b + 1) * BLOCK)
        decayed.append((kf[s] * jnp.exp((running - starts[b]) - parts[b])).astype(BF16))
    decayed = jnp.concatenate(decayed, axis=0)
    v = project(2 * kw, 2 * kw + vw)
    val[...] = v
    dv = send.shape[0] - EXTRA_ROWS
    states = []
    for g in range(vw // 256):
        m = lax.dot_general(
            v[:, g * 256 : (g + 1) * 256],
            decayed[:, g * 128 : (g + 1) * 128],
            TN,
            preferred_element_type=F32,
        )
        states.append(fold(m, dv))
    pack(send, jnp.concatenate(states, axis=1), jnp.exp(running))


def fold(m, dv):
    step = m.shape[1] // (m.shape[0] // dv)
    lane = lax.broadcasted_iota(jnp.int32, (dv, m.shape[1]), 1) // step
    out = m[:dv]
    for h in range(1, m.shape[0] // dv):
        out = jnp.where(lane == h, m[h * dv : (h + 1) * dv], out)
    return out


def pack(ref, state, decay, halo=None):
    dv = state.shape[0]
    ref[:dv, :] = state.astype(BF16)
    top = decay.astype(BF16).astype(F32)
    row = lax.broadcasted_iota(jnp.int32, (EXTRA_ROWS, state.shape[1]), 0)
    tail = jnp.where(row == 0, top, decay - top)
    if halo is not None:
        tail = jnp.where(row < 2, tail, halo)
    ref[dv:, :] = tail.astype(BF16)


def unpack(v, dv):
    tail = v[dv:].astype(F32)
    return v[:dv].astype(F32), tail[0:1] + tail[1:2], tail


def to_tail(last):
    width = last.shape[1] // 2
    row = lax.broadcasted_iota(jnp.int32, (EXTRA_ROWS, width), 0)
    tail = jnp.zeros((EXTRA_ROWS, width), F32)
    end = last.shape[0]
    for i in range(4):
        at = end - 2 + i // 2
        part = last[at : at + 1, (i % 2) * width : (i % 2 + 1) * width]
        tail = jnp.where(row == 2 + i, part, tail)
    return tail


def from_tail(tail):
    return jnp.concatenate(
        [
            jnp.concatenate([tail[2:3], tail[3:4]], axis=1),
            jnp.concatenate([tail[4:5], tail[5:6]], axis=1),
        ],
        axis=0,
    )


def fill(stack, items):
    for i, item in enumerate(items):
        stack[i] = item[...]


def halo_of_round(halo, stack, radix, stride, digit, dv):
    low_zero = lax.rem(lax.axis_index("sp"), stride) == 0
    for j in range(radix - 1):
        tail = stack[j ^ digit][dv:].astype(F32)
        halo = jnp.where((j + 1 == digit) & low_zero, tail, halo)
    return halo


def before_round(pre, dv, lanes):
    if pre is None:
        return (
            jnp.zeros((dv, lanes), F32),
            jnp.ones((1, lanes), F32),
            jnp.zeros((EXTRA_ROWS, lanes), F32),
        )
    return unpack(pre[...], dv)


def join_round(radix, stride, *refs):
    items, pre, (send, pre_out, stack) = refs[:radix], refs[radix:-3], refs[-3:]
    dv = send.shape[0] - EXTRA_ROWS
    fill(stack, items)
    digit = lax.rem(lax.axis_index("sp") // stride, radix)
    lanes = stack.shape[2]
    had_s, had_d, had_halo = before_round(pre[0] if pre else None, dv, lanes)
    pre_s, pre_d = jnp.zeros((dv, lanes), F32), jnp.ones((1, lanes), F32)
    tot_s, tot_d = pre_s, pre_d
    for j in range(radix):
        s, d, tail = unpack(stack[j ^ digit], dv)
        before = j < digit
        pre_s = jnp.where(before, d * pre_s + s, pre_s)
        pre_d = jnp.where(before, d * pre_d, pre_d)
        tot_s, tot_d = d * tot_s + s, d * tot_d
    halo = halo_of_round(had_halo, stack, radix, stride, digit, dv)
    pack(pre_out, had_d * pre_s + had_s, had_d * pre_d, halo)
    pack(send, tot_s, tot_d, tail)


def scaled(x, w, r):
    s = dot(x, w)
    return (s * tile_lanes(r, s.shape[1])).astype(BF16)


def conv_inputs(full, scale, wc, wh, send, prod, out):
    r = scale[...]
    x = full[...]
    p = scaled(x, wc[...], r).astype(F32) * scaled(x, wh[...], r).astype(F32)
    p = p.astype(BF16)
    prod[...] = p
    dv = send.shape[0] - EXTRA_ROWS
    tail = to_tail(p[p.shape[0] - 16 :].astype(F32))
    row = lax.broadcasted_iota(jnp.int32, tail.shape, 0)
    out[:dv, :] = send[:dv, :]
    out[dv:, :] = jnp.where(row < 2, send[dv:, :].astype(F32), tail).astype(BF16)


def late_half(full, scale, taps, wb, wq, prod, query, outer, conv):
    r = scale[...]
    x = full[...]
    b = scaled(x, wb[...], r)
    outer[...] = b
    p = prod[...].astype(F32)
    row = lax.broadcasted_iota(jnp.int32, p.shape, 0)
    t = taps[...].astype(F32)
    total = jnp.zeros(p.shape, F32)
    for j in range(taps.shape[0] - 1):
        back = taps.shape[0] - 1 - j
        total = total + t[j : j + 1] * jnp.where(row >= back, pltpu.roll(p, back, 0), 0.0)
    total = total + t[taps.shape[0] - 1 :] * p
    conv[...] = (b.astype(F32) * total).astype(BF16)
    query[...] = scaled(x, wq[...], r)


def blockwise(
    key_dim, query, key, val, cum, base, start, full, scale, wg, gain, raw, through, first, gate
):
    rows = query.shape[0]
    n = rows // BLOCK
    shrink = key_dim**-0.5
    first[...] = start[...].T
    gated = scaled(full[...], wg[...], scale[...]).astype(F32)
    gate[...] = gated * jax.nn.sigmoid(gated) * tile_lanes(gain[...], gated.shape[1])
    k_mask = block_mask(256, 64, 128, 32)
    v_mask = block_mask(256, 64, 256, 64)
    causal = lax.broadcasted_iota(jnp.int32, (BLOCK, 256), 0) >= (
        lax.broadcasted_iota(jnp.int32, (BLOCK, 256), 1) % BLOCK
    )
    zero = jnp.zeros((), BF16)
    for g in range(val.shape[1] // 256):
        kl = slice(g * 128, (g + 1) * 128)
        vl = slice(g * 256, (g + 1) * 256)
        state = None
        for b in range(n):
            s = slice(b * BLOCK, (b + 1) * BLOCK)
            c = cum[s, kl]
            q = query[s, kl].astype(F32) * shrink
            k = key[s, kl].astype(F32)
            end = c[BLOCK - 1 :]
            q_in = (q * jnp.exp(c)).astype(BF16)
            k_in = (k * jnp.exp(-c)).astype(BF16)
            through[s, kl] = (q * jnp.exp(c + base[b : b + 1, kl])).astype(BF16)
            v = val[s, vl]
            k_wide = jnp.where(k_mask, jnp.concatenate([k_in] * 4, axis=0), zero)
            scores = lax.dot_general(q_in, k_wide, NT, preferred_element_type=F32)
            scores = jnp.where(causal, scores, 0.0).astype(BF16)
            v_wide = jnp.where(v_mask, jnp.concatenate([v] * 4, axis=0), zero)
            out = dot(scores, v_wide)
            if state is not None:
                out = out + lax.dot_general(
                    q_in, state.astype(BF16), NT, preferred_element_type=F32
                )
            raw[s, vl] = out
            if b < n - 1:
                k_out = (k * jnp.exp(end - c)).astype(BF16)
                new = lax.dot_general(v, k_out, TN, preferred_element_type=F32)
                new = jnp.where(k_mask, new, 0.0)
                state = new if state is None else state * jnp.exp(end) + new


def rows_out(half, incoming, halo, raw, through, gate, conv, outer, prod, taps):
    rows = raw.shape[0] // 2
    at = pl.multiple_of(half * rows, 64)
    here = pl.ds(at, rows)
    ones = block_mask(256, 64, 256, 64).astype(BF16) * (1.0 / 64)
    ones = ones.astype(BF16)
    parts = []
    for g in range(raw.shape[1] // 256):
        vl = slice(g * 256, (g + 1) * 256)
        x = raw[here, vl] + lax.dot_general(
            through[here, g * 128 : (g + 1) * 128],
            incoming[g],
            NT,
            preferred_element_type=F32,
        )
        mean = dot((x * x).astype(BF16), ones)
        parts.append((x * lax.rsqrt(mean + NORM_EPS) * gate[here, vl]).astype(BF16))
    attn = jnp.concatenate(parts, axis=1)
    p = prod[:16, :].astype(F32)
    row = lax.broadcasted_iota(jnp.int32, p.shape, 0)
    t = taps[...].astype(F32)
    back2 = jnp.where(row == 0, halo[0:1], jnp.where(row == 1, halo[1:2], pltpu.roll(p, 2, 0)))
    back1 = jnp.where(row == 0, halo[1:2], pltpu.roll(p, 1, 0))
    top = outer[:16, :].astype(F32) * (t[0:1] * back2 + t[1:2] * back1 + t[2:3] * p)
    mine = conv[here, :]
    head = jnp.where(half == 0, top, mine[:16].astype(F32)).astype(BF16)
    left = jnp.concatenate([head, mine[16:]], axis=0)
    return left, attn


def project_out(left, attn, wc, wa, out, skip=0):
    step = 512
    for n in range(0, out.shape[1], step):
        at = slice(skip + n, skip + n + step)
        s = dot(left, wc[:, at]) + dot(attn, wa[:, at])
        out[:, n : n + step] = s.astype(out.dtype)


def partner_rows(radix, stride, *refs):
    items, pre = refs[:radix], refs[radix:-16]
    first, raw, through, gate, conv, outer, prod, taps, wc, wa = refs[-16:-6]
    out, left_out, attn_out, state, halo_out, stack = refs[-6:]
    dv = first.shape[0]
    fill(stack, items)
    digit = lax.rem(lax.axis_index("sp") // stride, radix)
    lanes = stack.shape[2]
    had_s, had_d, had_halo = before_round(pre[0] if pre else None, dv, lanes)
    pre_s = first[...]
    for j in range(radix - 1):
        s, d, _ = unpack(stack[j ^ digit], dv)
        pre_s = jnp.where(j < digit, d * pre_s + s, pre_s)
    pre_s = had_d * pre_s + had_s
    mask = block_mask(256, 64, 128, 32)
    incoming = []
    for g in range(lanes // 128):
        s = pre_s[:, g * 128 : (g + 1) * 128]
        wide = jnp.where(mask, jnp.concatenate([s] * 4, axis=0), 0.0).astype(BF16)
        incoming.append(wide)
        state[g] = wide
    halo = from_tail(halo_of_round(had_halo, stack, radix, stride, digit, dv))
    halo_out[...] = jnp.concatenate([halo] * 4, axis=0)
    half = 1 - lax.axis_index("tp")
    left, attn = rows_out(half, incoming, halo, raw, through, gate, conv, outer, prod, taps)
    left_out[...] = left
    attn_out[...] = attn
    project_out(left, attn, wc, wa, out)


def partner_rest(left, attn, wc, wa, out):
    project_out(left[...], attn[...], wc, wa, out, out.shape[1])


def add_rows(mine, first, second, out_hbm, buf, sems):
    chunks = buf.shape[0]
    rows = buf.shape[1]
    width = first.shape[1]
    copies = []
    for i in range(chunks):
        here = slice(i * rows, (i + 1) * rows)
        buf[i, :, :width] = (mine[here, :width] + first[here, :].astype(F32)).astype(BF16)
        buf[i, :, width:] = (mine[here, width:] + second[here, :].astype(F32)).astype(BF16)
        copies.append(pltpu.make_async_copy(buf.at[i], out_hbm.at[here, :], sems.at[i]))
        copies[-1].start()
    for c in copies:
        c.wait()


def own_rows(state, halo, raw, through, gate, conv, outer, prod, taps, wc, wa, out):
    incoming = [state[g] for g in range(state.shape[0])]
    half = lax.axis_index("tp")
    left, attn = rows_out(
        half, incoming, halo[0:2, :], raw, through, gate, conv, outer, prod, taps
    )
    project_out(left, attn, wc, wa, out)


def radices(n):
    found = []
    while n > 1:
        r = 4 if n % 4 == 0 else 2
        found.append(r)
        n //= r
    return found


def on_device(
    tokens,
    input_norm_gain,
    outer_gate_weight,
    inner_gate_weight,
    convolution_input_weight,
    convolution_kernel_taps,
    query_weight_matrix,
    key_weight_matrix,
    value_weight_matrix,
    forget_gate_weight,
    attention_gate_weight,
    forget_gate_bias,
    extra_logarithm_decay,
    initial_head_state,
    head_norm_gain,
    convolution_output_weight,
    attention_output_weight,
):
    rows, half = tokens.shape
    heads, dk, dv = initial_head_state.shape
    kw, vw, cw = heads * dk, heads * dv, outer_gate_weight.shape[1]
    model = convolution_output_weight.shape[1]
    n_sp = lax.axis_size("sp")
    swap = [(0, 1), (1, 0)]
    other = lax.ppermute(tokens, "tp", swap)
    gain = input_norm_gain.reshape(1, -1)
    early = (key_weight_matrix, forget_gate_weight, value_weight_matrix)
    width = sum(w.shape[1] for w in early)
    extra = extra_logarithm_decay.T
    flops = 2 * rows * half * width
    acc, xg, ssq, wide, ahead = call(
        own_half,
        [
            ((rows, width), F32),
            ((rows, half), BF16),
            ((rows, 128), F32),
            ((rows, kw), F32),
            ((half, width), BF16),
        ],
        [(tokens, HBM), (gain, HBM), (extra, HBM)] + [(w, HBM) for w in early],
        flops,
        [
            pltpu.VMEM((half, width), BF16),
            pltpu.SemaphoreType.DMA((2, len(early))),
            pltpu.VMEM(tokens.shape, BF16),
            pltpu.VMEM(gain.shape, F32),
            pltpu.VMEM(extra.shape, F32),
            pltpu.SemaphoreType.DMA((3,)),
        ],
    )
    full, scale, key, val, cum, base, send = call(
        other_half,
        [
            ((rows, 2 * half), BF16),
            ((rows, 128), F32),
            ((rows, kw), BF16),
            ((rows, vw), BF16),
            ((rows, kw), F32),
            ((8, kw), F32),
            ((dv + EXTRA_ROWS, kw), BF16),
        ],
        [(other, VMEM), (gain, VMEM), (forget_gate_bias.reshape(1, -1), VMEM)]
        + [(a, VMEM) for a in (acc, xg, ssq, wide, ahead)],
        flops,
    )
    prod, send_halo = call(
        conv_inputs,
        [((rows, cw), BF16), (send.shape, BF16)],
        [(a, VMEM) for a in (full, scale, inner_gate_weight, convolution_input_weight, send)],
        2 * rows * 2 * half * 2 * cw,
    )
    query, outer, conv = call(
        late_half,
        [((rows, kw), BF16), ((rows, cw), BF16), ((rows, cw), BF16)],
        [
            (a, VMEM)
            for a in (
                full,
                scale,
                convolution_kernel_taps,
                outer_gate_weight,
                query_weight_matrix,
                prod,
            )
        ],
        2 * rows * 2 * half * (kw + cw),
    )
    raw, through, first, gate = call(
        functools.partial(blockwise, dk),
        [((rows, vw), F32), ((rows, kw), BF16), ((dv, kw), F32), ((rows, vw), F32)],
        [
            (a, VMEM)
            for a in (
                query,
                key,
                val,
                cum,
                base,
                initial_head_state.reshape(heads * dk, dv),
                full,
                scale,
                attention_gate_weight,
                head_norm_gain.reshape(1, -1),
            )
        ],
        2 * rows * 2 * half * (kw + vw),
    )
    pre = ()
    stride = 1
    plan = radices(n_sp)
    crossed = len(plan) % 2 == 0
    for turn, radix in enumerate(plan):
        items = [send] + [None] * (radix - 1)
        for j in FIRST if turn == 0 else LAST if radix == 4 else range(1, radix):
            pairs = [
                (2 * i + c, 2 * (i ^ (j * stride)) + (1 - c if crossed else c))
                for i in range(n_sp)
                for c in range(2)
            ]
            payload = send_halo if turn == 0 and j % 2 == 1 else send
            items[j] = lax.ppermute(payload, ("sp", "tp"), pairs)
        if crossed and turn < len(plan) - 1:
            items[0] = lax.ppermute(send, "tp", swap)
        if crossed and turn > 0:
            pre = (lax.ppermute(pre[0], "tp", swap),)
        stack = [pltpu.VMEM((radix,) + send.shape, BF16)]
        if turn < len(plan) - 1:
            send, *pre = call(
                functools.partial(join_round, radix, stride),
                [(send.shape, BF16), (send.shape, BF16)],
                [(a, VMEM) for a in (*items, *pre)],
                1 << 20,
                stack,
            )
            stride *= radix
    tail = [
        (a, VMEM)
        for a in (
            raw,
            through,
            gate,
            conv,
            outer,
            prod,
            convolution_kernel_taps,
            convolution_output_weight,
            attention_output_weight,
        )
    ]
    flops = 2 * (rows // 2) * model * (vw + cw)
    theirs, left, attn, state, halo = call(
        functools.partial(partner_rows, plan[-1], stride),
        [
            ((rows // 2, model // 2), BF16),
            ((rows // 2, cw), BF16),
            ((rows // 2, vw), BF16),
            ((kw // 128, 256, 128), BF16),
            ((8, cw), F32),
        ],
        [(a, VMEM) for a in (*items, *pre, first)] + tail,
        flops // 2,
        stack,
    )
    got_first = lax.ppermute(theirs, "tp", swap)
    (theirs,) = call(
        partner_rest,
        [((rows // 2, model // 2), BF16)],
        [
            (a, VMEM)
            for a in (left, attn, convolution_output_weight, attention_output_weight)
        ],
        flops // 2,
    )
    got_second = lax.ppermute(theirs, "tp", swap)
    (mine,) = call(
        own_rows, [((rows // 2, model), F32)], [(state, VMEM), (halo, VMEM)] + tail, flops
    )
    return pl.pallas_call(
        add_rows,
        out_shape=jax.ShapeDtypeStruct((rows // 2, model), BF16),
        in_specs=[VMEM] * 3,
        out_specs=HBM,
        scratch_shapes=[
            pltpu.VMEM((CHUNKS, rows // 2 // CHUNKS, model), BF16),
            pltpu.SemaphoreType.DMA((CHUNKS,)),
        ],
        compiler_params=pltpu.CompilerParams(vmem_limit_bytes=12 << 20),
        cost_estimate=pl.CostEstimate(flops=1 << 20, bytes_accessed=1 << 20, transcendentals=0),
        name="add_rows",
    )(mine, got_first, got_second)


def solution(mesh):
    placed = (
        P("sp", "tp"),
        P(),
        P(None, "tp"),
        P(None, "tp"),
        P(None, "tp"),
        P(None, "tp"),
        P(None, "tp"),
        P(None, "tp"),
        P(None, "tp"),
        P(None, "tp"),
        P(None, "tp"),
        P("tp"),
        P("sp", "tp"),
        P("tp", None, None),
        P(),
        P("tp", None),
        P("tp", None),
    )

    return jax.shard_map(
        on_device, mesh=mesh, in_specs=placed, out_specs=P(("sp", "tp"), None), check_vma=False
    )
```

```python
import functools

import jax
import jax.numpy as jnp
from jax import lax
from jax.experimental import pallas as pl
from jax.experimental.pallas import tpu as pltpu
from jax.sharding import PartitionSpec as P


BLOCK = 64
NORM_EPS = 1e-06
GATE_SOFTNESS = 16.0
F32 = jnp.float32
BF16 = jnp.bfloat16
NT = (((1,), (1,)), ((), ()))
TN = (((0,), (0,)), ((), ()))
VMEM = pl.BlockSpec(memory_space=pltpu.VMEM)
HBM = pl.BlockSpec(memory_space=pltpu.HBM)
EXTRA_ROWS = 8
CHUNKS = 4
FIRST = (2, 3, 1)
LAST = (3, 2, 1)


def dot(a, b):
    return jnp.dot(a, b, preferred_element_type=F32)


def call(body, outs, ins, flops, scratch=(), limit=12 << 20):
    specs = [s for _, s in ins]
    return pl.pallas_call(
        body,
        out_shape=[jax.ShapeDtypeStruct(s, d) for s, d in outs],
        in_specs=specs,
        out_specs=[VMEM] * len(outs),
        scratch_shapes=list(scratch),
        compiler_params=pltpu.CompilerParams(vmem_limit_bytes=limit),
        cost_estimate=pl.CostEstimate(flops=flops, bytes_accessed=1 << 20, transcendentals=0),
    )(*[pltpu.with_memory_space_constraint(a, pltpu.HBM) if s is HBM else a for a, s in ins])


def weight_copies(hbm, buf, sems, row, rows):
    copies, at = [], 0
    for i, w in enumerate(hbm):
        cols = w.shape[1]
        copies.append(
            pltpu.make_async_copy(
                w.at[pl.ds(row, rows), :], buf.at[:, at : at + cols], sems.at[i]
            )
        )
        at += cols
    return copies


def tile_lanes(column, lanes):
    return jnp.concatenate([column] * (lanes // column.shape[1]), axis=1)


def block_mask(rows, row_step, lanes, lane_step):
    r = lax.broadcasted_iota(jnp.int32, (rows, lanes), 0) // row_step
    c = lax.broadcasted_iota(jnp.int32, (rows, lanes), 1) // lane_step
    return r == c


def own_half(tok_hbm, gain_hbm, extra_hbm, *refs):
    n = len(refs) - 11
    weights, (acc, xg, ssq, wide, ahead) = refs[:n], refs[n : n + 5]
    buf, sems, tok, gain, extra, small = refs[n + 5 :]
    tp = lax.axis_index("tp")
    half = tok.shape[1]
    here = pl.multiple_of(tp * half, half)
    away = pl.multiple_of((1 - tp) * half, half)
    loads = [
        pltpu.make_async_copy(src, dst, small.at[i])
        for i, (src, dst) in enumerate([(extra_hbm, extra), (gain_hbm, gain), (tok_hbm, tok)])
    ]
    copies = weight_copies(weights, buf, sems.at[0], here, half)
    more = weight_copies(weights, ahead, sems.at[1], away, half)
    for c in loads + copies:
        c.start()
    loads[0].wait()
    loads[1].wait()
    loads[2].wait()
    for c in more:
        c.start()
    for c in copies:
        c.wait()
    heads = extra.shape[0]
    lanes = wide.shape[1]
    r = lax.broadcasted_iota(jnp.int32, (heads, lanes), 0)
    c = lax.broadcasted_iota(jnp.int32, (heads, lanes), 1) // (lanes // heads)
    wide[...] = lax.dot_general(
        extra[...],
        (r == c).astype(F32),
        TN,
        precision=lax.Precision.HIGHEST,
        preferred_element_type=F32,
    )
    x = tok[...].astype(F32)
    ssq[...] = jnp.broadcast_to(jnp.sum(x * x, axis=1, keepdims=True), ssq.shape)
    left = (x * gain[:, pl.ds(here, half)]).astype(BF16)
    xg[...] = left
    acc[...] = dot(left, buf[...])
    for c in more:
        c.wait()


def other_half(
    tok, gain, bias, acc, xg, ssq, wide, wnext, full, scale, key, val, cum, base, send
):
    tp = lax.axis_index("tp")
    rows, half = tok.shape
    here = pl.multiple_of(tp * half, half)
    away = pl.multiple_of((1 - tp) * half, half)
    x = tok[...].astype(F32)
    power = (ssq[:, :1] + jnp.sum(x * x, axis=1, keepdims=True)) * (0.5 / half)
    r = jnp.broadcast_to(lax.rsqrt(power + NORM_EPS), scale.shape)
    scale[...] = r
    left = (x * gain[:, pl.ds(away, half)]).astype(BF16)
    full[:, pl.ds(away, half)] = left
    full[:, pl.ds(here, half)] = xg[...]

    def project(lo, hi):
        s = acc[:, lo:hi] + dot(left, wnext[:, lo:hi])
        return (s * tile_lanes(r, hi - lo)).astype(BF16)

    kw, vw = key.shape[1], val.shape[1]
    k = project(0, kw)
    key[...] = k
    f = project(kw, 2 * kw).astype(F32) + bias[...]
    log = (jnp.minimum(f, 0.0) - jnp.log1p(jnp.exp(-jnp.abs(f)))) * (1.0 / GATE_SOFTNESS)
    log = log + wide[...]
    hi = log.astype(BF16)
    rest = log - hi.astype(F32)
    mid = rest.astype(BF16)
    low = (rest - mid.astype(F32)).astype(BF16)
    tri = (
        lax.broadcasted_iota(jnp.int32, (BLOCK, 3 * BLOCK), 0)
        >= lax.broadcasted_iota(jnp.int32, (BLOCK, 3 * BLOCK), 1) % BLOCK
    ).astype(BF16)
    n = rows // BLOCK
    running = jnp.zeros((1, kw), F32)
    starts, parts = [], []
    for b in range(n):
        s = slice(b * BLOCK, (b + 1) * BLOCK)
        part = dot(tri, jnp.concatenate([hi[s], mid[s], low[s]], axis=0))
        cum[s, :] = part
        parts.append(part)
        starts.append(running)
        running = running + part[BLOCK - 1 :]
    base[...] = jnp.concatenate(starts + [running] * (base.shape[0] - n), axis=0)
    kf = k.astype(F32)
    decayed = []
    for b in range(n):
        s = slice(b * BLOCK, (b + 1) * BLOCK)
        decayed.append((kf[s] * jnp.exp((running - starts[b]) - parts[b])).astype(BF16))
    decayed = jnp.concatenate(decayed, axis=0)
    v = project(2 * kw, 2 * kw + vw)
    val[...] = v
    dv = send.shape[0] - EXTRA_ROWS
    states = []
    for g in range(vw // 256):
        m = lax.dot_general(
            v[:, g * 256 : (g + 1) * 256],
            decayed[:, g * 128 : (g + 1) * 128],
            TN,
            preferred_element_type=F32,
        )
        states.append(fold(m, dv))
    pack(send, jnp.concatenate(states, axis=1), jnp.exp(running))


def fold(m, dv):
    step = m.shape[1] // (m.shape[0] // dv)
    lane = lax.broadcasted_iota(jnp.int32, (dv, m.shape[1]), 1) // step
    out = m[:dv]
    for h in range(1, m.shape[0] // dv):
        out = jnp.where(lane == h, m[h * dv : (h + 1) * dv], out)
    return out


def pack(ref, state, decay, halo=None):
    dv = state.shape[0]
    ref[:dv, :] = state.astype(BF16)
    top = decay.astype(BF16).astype(F32)
    row = lax.broadcasted_iota(jnp.int32, (EXTRA_ROWS, state.shape[1]), 0)
    tail = jnp.where(row == 0, top, decay - top)
    if halo is not None:
        tail = jnp.where(row < 2, tail, halo)
    ref[dv:, :] = tail.astype(BF16)


def unpack(v, dv):
    tail = v[dv:].astype(F32)
    return v[:dv].astype(F32), tail[0:1] + tail[1:2], tail


def to_tail(last):
    width = last.shape[1] // 2
    row = lax.broadcasted_iota(jnp.int32, (EXTRA_ROWS, width), 0)
    tail = jnp.zeros((EXTRA_ROWS, width), F32)
    end = last.shape[0]
    for i in range(4):
        at = end - 2 + i // 2
        part = last[at : at + 1, (i % 2) * width : (i % 2 + 1) * width]
        tail = jnp.where(row == 2 + i, part, tail)
    return tail


def from_tail(tail):
    return jnp.concatenate(
        [
            jnp.concatenate([tail[2:3], tail[3:4]], axis=1),
            jnp.concatenate([tail[4:5], tail[5:6]], axis=1),
        ],
        axis=0,
    )


def fill(stack, items):
    for i, item in enumerate(items):
        stack[i] = item[...]


def halo_of_round(halo, stack, radix, stride, digit, dv):
    low_zero = lax.rem(lax.axis_index("sp"), stride) == 0
    for j in range(radix - 1):
        tail = stack[j ^ digit][dv:].astype(F32)
        halo = jnp.where((j + 1 == digit) & low_zero, tail, halo)
    return halo


def before_round(pre, dv, lanes):
    if pre is None:
        return (
            jnp.zeros((dv, lanes), F32),
            jnp.ones((1, lanes), F32),
            jnp.zeros((EXTRA_ROWS, lanes), F32),
        )
    return unpack(pre[...], dv)


def join_round(radix, stride, *refs):
    items, pre, (send, pre_out, stack) = refs[:radix], refs[radix:-3], refs[-3:]
    dv = send.shape[0] - EXTRA_ROWS
    fill(stack, items)
    digit = lax.rem(lax.axis_index("sp") // stride, radix)
    lanes = stack.shape[2]
    had_s, had_d, had_halo = before_round(pre[0] if pre else None, dv, lanes)
    pre_s, pre_d = jnp.zeros((dv, lanes), F32), jnp.ones((1, lanes), F32)
    tot_s, tot_d = pre_s, pre_d
    for j in range(radix):
        s, d, tail = unpack(stack[j ^ digit], dv)
        before = j < digit
        pre_s = jnp.where(before, d * pre_s + s, pre_s)
        pre_d = jnp.where(before, d * pre_d, pre_d)
        tot_s, tot_d = d * tot_s + s, d * tot_d
    halo = halo_of_round(had_halo, stack, radix, stride, digit, dv)
    pack(pre_out, had_d * pre_s + had_s, had_d * pre_d, halo)
    pack(send, tot_s, tot_d, tail)


def scaled(x, w, r):
    s = dot(x, w)
    return (s * tile_lanes(r, s.shape[1])).astype(BF16)


def conv_product(full, scale, wc, wh, rows):
    r = scale[rows, :]
    x = full[rows, :]
    p = scaled(x, wc[...], r).astype(F32) * scaled(x, wh[...], r).astype(F32)
    return p.astype(BF16)


def conv_halo(full, scale, wc, wh, send, out):
    rows = full.shape[0]
    p = conv_product(full, scale, wc, wh, slice(rows - 16, rows))
    dv = send.shape[0] - EXTRA_ROWS
    tail = to_tail(p.astype(F32))
    row = lax.broadcasted_iota(jnp.int32, tail.shape, 0)
    out[:dv, :] = send[:dv, :]
    out[dv:, :] = jnp.where(row < 2, send[dv:, :].astype(F32), tail).astype(BF16)


def conv_inputs(full, scale, wc, wh, wg, gain, prod, gate):
    prod[...] = conv_product(full, scale, wc, wh, slice(0, full.shape[0]))
    gated = scaled(full[...], wg[...], scale[...]).astype(F32)
    gate[...] = gated * jax.nn.sigmoid(gated) * tile_lanes(gain[...], gated.shape[1])


def late_half(full, scale, taps, wb, wq, prod, query, outer, conv):
    r = scale[...]
    x = full[...]
    b = scaled(x, wb[...], r)
    outer[...] = b
    p = prod[...].astype(F32)
    row = lax.broadcasted_iota(jnp.int32, p.shape, 0)
    t = taps[...].astype(F32)
    total = jnp.zeros(p.shape, F32)
    for j in range(taps.shape[0] - 1):
        back = taps.shape[0] - 1 - j
        total = total + t[j : j + 1] * jnp.where(row >= back, pltpu.roll(p, back, 0), 0.0)
    total = total + t[taps.shape[0] - 1 :] * p
    conv[...] = (b.astype(F32) * total).astype(BF16)
    query[...] = scaled(x, wq[...], r)


def blockwise(
    key_dim, query, key, val, cum, base, start, raw, through, first
):
    rows = query.shape[0]
    n = rows // BLOCK
    shrink = key_dim**-0.5
    first[...] = start[...].T
    k_mask = block_mask(256, 64, 128, 32)
    v_mask = block_mask(256, 64, 256, 64)
    causal = lax.broadcasted_iota(jnp.int32, (BLOCK, 256), 0) >= (
        lax.broadcasted_iota(jnp.int32, (BLOCK, 256), 1) % BLOCK
    )
    zero = jnp.zeros((), BF16)
    for g in range(val.shape[1] // 256):
        kl = slice(g * 128, (g + 1) * 128)
        vl = slice(g * 256, (g + 1) * 256)
        state = None
        for b in range(n):
            s = slice(b * BLOCK, (b + 1) * BLOCK)
            c = cum[s, kl]
            q = query[s, kl].astype(F32) * shrink
            k = key[s, kl].astype(F32)
            end = c[BLOCK - 1 :]
            q_in = (q * jnp.exp(c)).astype(BF16)
            k_in = (k * jnp.exp(-c)).astype(BF16)
            through[s, kl] = (q * jnp.exp(c + base[b : b + 1, kl])).astype(BF16)
            v = val[s, vl]
            k_wide = jnp.where(k_mask, jnp.concatenate([k_in] * 4, axis=0), zero)
            scores = lax.dot_general(q_in, k_wide, NT, preferred_element_type=F32)
            scores = jnp.where(causal, scores, 0.0).astype(BF16)
            v_wide = jnp.where(v_mask, jnp.concatenate([v] * 4, axis=0), zero)
            out = dot(scores, v_wide)
            if state is not None:
                out = out + lax.dot_general(
                    q_in, state.astype(BF16), NT, preferred_element_type=F32
                )
            raw[s, vl] = out
            if b < n - 1:
                k_out = (k * jnp.exp(end - c)).astype(BF16)
                new = lax.dot_general(v, k_out, TN, preferred_element_type=F32)
                new = jnp.where(k_mask, new, 0.0)
                state = new if state is None else state * jnp.exp(end) + new


def rows_out(half, incoming, halo, raw, through, gate, conv, outer, prod, taps):
    rows = raw.shape[0] // 2
    at = pl.multiple_of(half * rows, 64)
    here = pl.ds(at, rows)
    ones = block_mask(256, 64, 256, 64).astype(BF16) * (1.0 / 64)
    ones = ones.astype(BF16)
    parts = []
    for g in range(raw.shape[1] // 256):
        vl = slice(g * 256, (g + 1) * 256)
        x = raw[here, vl] + lax.dot_general(
            through[here, g * 128 : (g + 1) * 128],
            incoming[g],
            NT,
            preferred_element_type=F32,
        )
        mean = dot((x * x).astype(BF16), ones)
        parts.append((x * lax.rsqrt(mean + NORM_EPS) * gate[here, vl]).astype(BF16))
    attn = jnp.concatenate(parts, axis=1)
    p = prod[:16, :].astype(F32)
    row = lax.broadcasted_iota(jnp.int32, p.shape, 0)
    t = taps[...].astype(F32)
    back2 = jnp.where(row == 0, halo[0:1], jnp.where(row == 1, halo[1:2], pltpu.roll(p, 2, 0)))
    back1 = jnp.where(row == 0, halo[1:2], pltpu.roll(p, 1, 0))
    top = outer[:16, :].astype(F32) * (t[0:1] * back2 + t[1:2] * back1 + t[2:3] * p)
    mine = conv[here, :]
    head = jnp.where(half == 0, top, mine[:16].astype(F32)).astype(BF16)
    left = jnp.concatenate([head, mine[16:]], axis=0)
    return left, attn


def project_out(left, attn, wc, wa, out, skip=0):
    step = 512
    for n in range(0, out.shape[1], step):
        at = slice(skip + n, skip + n + step)
        s = dot(left, wc[:, at]) + dot(attn, wa[:, at])
        out[:, n : n + step] = s.astype(out.dtype)


def partner_rows(radix, stride, *refs):
    items, pre = refs[:radix], refs[radix:-16]
    first, raw, through, gate, conv, outer, prod, taps, wc, wa = refs[-16:-6]
    out, left_out, attn_out, state, halo_out, stack = refs[-6:]
    dv = first.shape[0]
    fill(stack, items)
    digit = lax.rem(lax.axis_index("sp") // stride, radix)
    lanes = stack.shape[2]
    had_s, had_d, had_halo = before_round(pre[0] if pre else None, dv, lanes)
    pre_s = first[...]
    for j in range(radix - 1):
        s, d, _ = unpack(stack[j ^ digit], dv)
        pre_s = jnp.where(j < digit, d * pre_s + s, pre_s)
    pre_s = had_d * pre_s + had_s
    mask = block_mask(256, 64, 128, 32)
    incoming = []
    for g in range(lanes // 128):
        s = pre_s[:, g * 128 : (g + 1) * 128]
        wide = jnp.where(mask, jnp.concatenate([s] * 4, axis=0), 0.0).astype(BF16)
        incoming.append(wide)
        state[g] = wide
    halo = from_tail(halo_of_round(had_halo, stack, radix, stride, digit, dv))
    halo_out[...] = jnp.concatenate([halo] * 4, axis=0)
    half = 1 - lax.axis_index("tp")
    left, attn = rows_out(half, incoming, halo, raw, through, gate, conv, outer, prod, taps)
    left_out[...] = left
    attn_out[...] = attn
    project_out(left, attn, wc, wa, out)


def partner_rest(left, attn, wc, wa, out):
    project_out(left[...], attn[...], wc, wa, out, out.shape[1])


def add_rows(mine, first, second, out_hbm, buf, sems):
    chunks = buf.shape[0]
    rows = buf.shape[1]
    width = first.shape[1]
    copies = []
    for i in range(chunks):
        here = slice(i * rows, (i + 1) * rows)
        buf[i, :, :width] = (mine[here, :width] + first[here, :].astype(F32)).astype(BF16)
        buf[i, :, width:] = (mine[here, width:] + second[here, :].astype(F32)).astype(BF16)
        copies.append(pltpu.make_async_copy(buf.at[i], out_hbm.at[here, :], sems.at[i]))
        copies[-1].start()
    for c in copies:
        c.wait()


def own_rows(state, halo, raw, through, gate, conv, outer, prod, taps, wc, wa, out):
    incoming = [state[g] for g in range(state.shape[0])]
    half = lax.axis_index("tp")
    left, attn = rows_out(
        half, incoming, halo[0:2, :], raw, through, gate, conv, outer, prod, taps
    )
    project_out(left, attn, wc, wa, out)


def radices(n):
    found = []
    while n > 1:
        r = 4 if n % 4 == 0 else 2
        found.append(r)
        n //= r
    return found


def on_device(
    tokens,
    input_norm_gain,
    outer_gate_weight,
    inner_gate_weight,
    convolution_input_weight,
    convolution_kernel_taps,
    query_weight_matrix,
    key_weight_matrix,
    value_weight_matrix,
    forget_gate_weight,
    attention_gate_weight,
    forget_gate_bias,
    extra_logarithm_decay,
    initial_head_state,
    head_norm_gain,
    convolution_output_weight,
    attention_output_weight,
):
    rows, half = tokens.shape
    heads, dk, dv = initial_head_state.shape
    kw, vw, cw = heads * dk, heads * dv, outer_gate_weight.shape[1]
    model = convolution_output_weight.shape[1]
    n_sp = lax.axis_size("sp")
    swap = [(0, 1), (1, 0)]
    other = lax.ppermute(tokens, "tp", swap)
    gain = input_norm_gain.reshape(1, -1)
    early = (key_weight_matrix, forget_gate_weight, value_weight_matrix)
    width = sum(w.shape[1] for w in early)
    extra = extra_logarithm_decay.T
    flops = 2 * rows * half * width
    acc, xg, ssq, wide, ahead = call(
        own_half,
        [
            ((rows, width), F32),
            ((rows, half), BF16),
            ((rows, 128), F32),
            ((rows, kw), F32),
            ((half, width), BF16),
        ],
        [(tokens, HBM), (gain, HBM), (extra, HBM)] + [(w, HBM) for w in early],
        flops,
        [
            pltpu.VMEM((half, width), BF16),
            pltpu.SemaphoreType.DMA((2, len(early))),
            pltpu.VMEM(tokens.shape, BF16),
            pltpu.VMEM(gain.shape, F32),
            pltpu.VMEM(extra.shape, F32),
            pltpu.SemaphoreType.DMA((3,)),
        ],
    )
    full, scale, key, val, cum, base, send = call(
        other_half,
        [
            ((rows, 2 * half), BF16),
            ((rows, 128), F32),
            ((rows, kw), BF16),
            ((rows, vw), BF16),
            ((rows, kw), F32),
            ((8, kw), F32),
            ((dv + EXTRA_ROWS, kw), BF16),
        ],
        [(other, VMEM), (gain, VMEM), (forget_gate_bias.reshape(1, -1), VMEM)]
        + [(a, VMEM) for a in (acc, xg, ssq, wide, ahead)],
        flops,
    )
    (send_halo,) = call(
        conv_halo,
        [(send.shape, BF16)],
        [(a, VMEM) for a in (full, scale, inner_gate_weight, convolution_input_weight, send)],
        2 * rows * half * cw,
    )
    prod, gate = call(
        conv_inputs,
        [((rows, cw), BF16), ((rows, vw), F32)],
        [
            (a, VMEM)
            for a in (
                full,
                scale,
                inner_gate_weight,
                convolution_input_weight,
                attention_gate_weight,
                head_norm_gain.reshape(1, -1),
            )
        ],
        2 * rows * 2 * half * (2 * cw + vw),
    )
    query, outer, conv = call(
        late_half,
        [((rows, kw), BF16), ((rows, cw), BF16), ((rows, cw), BF16)],
        [
            (a, VMEM)
            for a in (
                full,
                scale,
                convolution_kernel_taps,
                outer_gate_weight,
                query_weight_matrix,
                prod,
            )
        ],
        2 * rows * 2 * half * (kw + cw),
    )
    raw, through, first = call(
        functools.partial(blockwise, dk),
        [((rows, vw), F32), ((rows, kw), BF16), ((dv, kw), F32)],
        [
            (a, VMEM)
            for a in (query, key, val, cum, base, initial_head_state.reshape(heads * dk, dv))
        ],
        1 << 24,
    )
    pre = ()
    stride = 1
    plan = radices(n_sp)
    crossed = len(plan) % 2 == 0
    for turn, radix in enumerate(plan):
        items = [send] + [None] * (radix - 1)
        for j in FIRST if turn == 0 else LAST if radix == 4 else range(1, radix):
            pairs = [
                (2 * i + c, 2 * (i ^ (j * stride)) + (1 - c if crossed else c))
                for i in range(n_sp)
                for c in range(2)
            ]
            payload = send_halo if turn == 0 and j % 2 == 1 else send
            items[j] = lax.ppermute(payload, ("sp", "tp"), pairs)
        if crossed and turn < len(plan) - 1:
            items[0] = lax.ppermute(send, "tp", swap)
        if crossed and turn > 0:
            pre = (lax.ppermute(pre[0], "tp", swap),)
        stack = [pltpu.VMEM((radix,) + send.shape, BF16)]
        if turn < len(plan) - 1:
            send, *pre = call(
                functools.partial(join_round, radix, stride),
                [(send.shape, BF16), (send.shape, BF16)],
                [(a, VMEM) for a in (*items, *pre)],
                1 << 20,
                stack,
            )
            stride *= radix
    tail = [
        (a, VMEM)
        for a in (
            raw,
            through,
            gate,
            conv,
            outer,
            prod,
            convolution_kernel_taps,
            convolution_output_weight,
            attention_output_weight,
        )
    ]
    flops = 2 * (rows // 2) * model * (vw + cw)
    theirs, left, attn, state, halo = call(
        functools.partial(partner_rows, plan[-1], stride),
        [
            ((rows // 2, model // 2), BF16),
            ((rows // 2, cw), BF16),
            ((rows // 2, vw), BF16),
            ((kw // 128, 256, 128), BF16),
            ((8, cw), F32),
        ],
        [(a, VMEM) for a in (*items, *pre, first)] + tail,
        flops // 2,
        stack,
    )
    got_first = lax.ppermute(theirs, "tp", swap)
    (theirs,) = call(
        partner_rest,
        [((rows // 2, model // 2), BF16)],
        [
            (a, VMEM)
            for a in (left, attn, convolution_output_weight, attention_output_weight)
        ],
        flops // 2,
    )
    got_second = lax.ppermute(theirs, "tp", swap)
    (mine,) = call(
        own_rows, [((rows // 2, model), F32)], [(state, VMEM), (halo, VMEM)] + tail, flops
    )
    return pl.pallas_call(
        add_rows,
        out_shape=jax.ShapeDtypeStruct((rows // 2, model), BF16),
        in_specs=[VMEM] * 3,
        out_specs=HBM,
        scratch_shapes=[
            pltpu.VMEM((CHUNKS, rows // 2 // CHUNKS, model), BF16),
            pltpu.SemaphoreType.DMA((CHUNKS,)),
        ],
        compiler_params=pltpu.CompilerParams(vmem_limit_bytes=12 << 20),
        cost_estimate=pl.CostEstimate(flops=1 << 20, bytes_accessed=1 << 20, transcendentals=0),
        name="add_rows",
    )(mine, got_first, got_second)


def solution(mesh):
    placed = (
        P("sp", "tp"),
        P(),
        P(None, "tp"),
        P(None, "tp"),
        P(None, "tp"),
        P(None, "tp"),
        P(None, "tp"),
        P(None, "tp"),
        P(None, "tp"),
        P(None, "tp"),
        P(None, "tp"),
        P("tp"),
        P("sp", "tp"),
        P("tp", None, None),
        P(),
        P("tp", None),
        P("tp", None),
    )

    return jax.shard_map(
        on_device, mesh=mesh, in_specs=placed, out_specs=P(("sp", "tp"), None), check_vma=False
    )
```

```python
import functools

import jax
import jax.numpy as jnp
from jax import lax
from jax.experimental import pallas as pl
from jax.experimental.pallas import tpu as pltpu
from jax.sharding import PartitionSpec as P


BLOCK = 64
NORM_EPS = 1e-06
GATE_SOFTNESS = 16.0
F32 = jnp.float32
BF16 = jnp.bfloat16
NT = (((1,), (1,)), ((), ()))
TN = (((0,), (0,)), ((), ()))
VMEM = pl.BlockSpec(memory_space=pltpu.VMEM)
HBM = pl.BlockSpec(memory_space=pltpu.HBM)
EXTRA_ROWS = 8
CHUNKS = 4
FIRST = (2, 3, 1)
LAST = (3, 2, 1)


def dot(a, b):
    return jnp.dot(a, b, preferred_element_type=F32)


def call(body, outs, ins, flops, scratch=(), limit=12 << 20):
    specs = [s for _, s in ins]
    return pl.pallas_call(
        body,
        out_shape=[jax.ShapeDtypeStruct(s, d) for s, d in outs],
        in_specs=specs,
        out_specs=[VMEM] * len(outs),
        scratch_shapes=list(scratch),
        compiler_params=pltpu.CompilerParams(vmem_limit_bytes=limit),
        cost_estimate=pl.CostEstimate(flops=flops, bytes_accessed=1 << 20, transcendentals=0),
    )(*[pltpu.with_memory_space_constraint(a, pltpu.HBM) if s is HBM else a for a, s in ins])


def weight_copies(hbm, buf, sems, row, rows):
    copies, at = [], 0
    for i, w in enumerate(hbm):
        cols = w.shape[1]
        copies.append(
            pltpu.make_async_copy(
                w.at[pl.ds(row, rows), :], buf.at[:, at : at + cols], sems.at[i]
            )
        )
        at += cols
    return copies


def tile_lanes(column, lanes):
    return jnp.concatenate([column] * (lanes // column.shape[1]), axis=1)


def block_mask(rows, row_step, lanes, lane_step):
    r = lax.broadcasted_iota(jnp.int32, (rows, lanes), 0) // row_step
    c = lax.broadcasted_iota(jnp.int32, (rows, lanes), 1) // lane_step
    return r == c


def own_half(tok_hbm, gain_hbm, extra_hbm, *refs):
    n = len(refs) - 11
    weights, (acc, xg, ssq, wide, ahead) = refs[:n], refs[n : n + 5]
    buf, sems, tok, gain, extra, small = refs[n + 5 :]
    tp = lax.axis_index("tp")
    half = tok.shape[1]
    here = pl.multiple_of(tp * half, half)
    away = pl.multiple_of((1 - tp) * half, half)
    loads = [
        pltpu.make_async_copy(src, dst, small.at[i])
        for i, (src, dst) in enumerate([(extra_hbm, extra), (gain_hbm, gain), (tok_hbm, tok)])
    ]
    copies = weight_copies(weights, buf, sems.at[0], here, half)
    more = weight_copies(weights, ahead, sems.at[1], away, half)
    for c in loads + copies:
        c.start()
    loads[0].wait()
    loads[1].wait()
    loads[2].wait()
    for c in more:
        c.start()
    for c in copies:
        c.wait()
    heads = extra.shape[0]
    lanes = wide.shape[1]
    r = lax.broadcasted_iota(jnp.int32, (heads, lanes), 0)
    c = lax.broadcasted_iota(jnp.int32, (heads, lanes), 1) // (lanes // heads)
    wide[...] = lax.dot_general(
        extra[...],
        (r == c).astype(F32),
        TN,
        precision=lax.Precision.HIGHEST,
        preferred_element_type=F32,
    )
    x = tok[...].astype(F32)
    ssq[...] = jnp.broadcast_to(jnp.sum(x * x, axis=1, keepdims=True), ssq.shape)
    left = (x * gain[:, pl.ds(here, half)]).astype(BF16)
    xg[...] = left
    acc[...] = dot(left, buf[...])
    for c in more:
        c.wait()


def other_half(
    tok, gain, bias, acc, xg, ssq, wide, wnext, full, scale, key, val, cum, base, send
):
    tp = lax.axis_index("tp")
    rows, half = tok.shape
    here = pl.multiple_of(tp * half, half)
    away = pl.multiple_of((1 - tp) * half, half)
    x = tok[...].astype(F32)
    power = (ssq[:, :1] + jnp.sum(x * x, axis=1, keepdims=True)) * (0.5 / half)
    r = jnp.broadcast_to(lax.rsqrt(power + NORM_EPS), scale.shape)
    scale[...] = r
    left = (x * gain[:, pl.ds(away, half)]).astype(BF16)
    full[:, pl.ds(away, half)] = left
    full[:, pl.ds(here, half)] = xg[...]

    def project(lo, hi):
        s = acc[:, lo:hi] + dot(left, wnext[:, lo:hi])
        return (s * tile_lanes(r, hi - lo)).astype(BF16)

    kw, vw = key.shape[1], val.shape[1]
    k = project(0, kw)
    key[...] = k
    f = project(kw, 2 * kw).astype(F32) + bias[...]
    log = (jnp.minimum(f, 0.0) - jnp.log1p(jnp.exp(-jnp.abs(f)))) * (1.0 / GATE_SOFTNESS)
    log = log + wide[...]
    hi = log.astype(BF16)
    rest = log - hi.astype(F32)
    mid = rest.astype(BF16)
    low = (rest - mid.astype(F32)).astype(BF16)
    tri = (
        lax.broadcasted_iota(jnp.int32, (BLOCK, 3 * BLOCK), 0)
        >= lax.broadcasted_iota(jnp.int32, (BLOCK, 3 * BLOCK), 1) % BLOCK
    ).astype(BF16)
    n = rows // BLOCK
    running = jnp.zeros((1, kw), F32)
    starts, parts = [], []
    for b in range(n):
        s = slice(b * BLOCK, (b + 1) * BLOCK)
        part = dot(tri, jnp.concatenate([hi[s], mid[s], low[s]], axis=0))
        cum[s, :] = part
        parts.append(part)
        starts.append(running)
        running = running + part[BLOCK - 1 :]
    base[...] = jnp.concatenate(starts + [running] * (base.shape[0] - n), axis=0)
    kf = k.astype(F32)
    decayed = []
    for b in range(n):
        s = slice(b * BLOCK, (b + 1) * BLOCK)
        decayed.append((kf[s] * jnp.exp((running - starts[b]) - parts[b])).astype(BF16))
    decayed = jnp.concatenate(decayed, axis=0)
    v = project(2 * kw, 2 * kw + vw)
    val[...] = v
    dv = send.shape[0] - EXTRA_ROWS
    states = []
    for g in range(vw // 256):
        m = lax.dot_general(
            decayed[:, g * 128 : (g + 1) * 128],
            v[:, g * 256 : (g + 1) * 256],
            TN,
            preferred_element_type=F32,
        ).T
        states.append(fold(m, dv))
    pack(send, jnp.concatenate(states, axis=1), jnp.exp(running))


def fold(m, dv):
    step = m.shape[1] // (m.shape[0] // dv)
    lane = lax.broadcasted_iota(jnp.int32, (dv, m.shape[1]), 1) // step
    out = m[:dv]
    for h in range(1, m.shape[0] // dv):
        out = jnp.where(lane == h, m[h * dv : (h + 1) * dv], out)
    return out


def pack(ref, state, decay, halo=None):
    dv = state.shape[0]
    ref[:dv, :] = state.astype(BF16)
    top = decay.astype(BF16).astype(F32)
    row = lax.broadcasted_iota(jnp.int32, (EXTRA_ROWS, state.shape[1]), 0)
    tail = jnp.where(row == 0, top, decay - top)
    if halo is not None:
        tail = jnp.where(row < 2, tail, halo)
    ref[dv:, :] = tail.astype(BF16)


def unpack(v, dv):
    tail = v[dv:].astype(F32)
    return v[:dv].astype(F32), tail[0:1] + tail[1:2], tail


def to_tail(last):
    width = last.shape[1] // 2
    row = lax.broadcasted_iota(jnp.int32, (EXTRA_ROWS, width), 0)
    tail = jnp.zeros((EXTRA_ROWS, width), F32)
    end = last.shape[0]
    for i in range(4):
        at = end - 2 + i // 2
        part = last[at : at + 1, (i % 2) * width : (i % 2 + 1) * width]
        tail = jnp.where(row == 2 + i, part, tail)
    return tail


def from_tail(tail):
    return jnp.concatenate(
        [
            jnp.concatenate([tail[2:3], tail[3:4]], axis=1),
            jnp.concatenate([tail[4:5], tail[5:6]], axis=1),
        ],
        axis=0,
    )


def fill(stack, items):
    for i, item in enumerate(items):
        stack[i] = item[...]


def halo_of_round(halo, stack, radix, stride, digit, dv):
    low_zero = lax.rem(lax.axis_index("sp"), stride) == 0
    for j in range(radix - 1):
        tail = stack[j ^ digit][dv:].astype(F32)
        halo = jnp.where((j + 1 == digit) & low_zero, tail, halo)
    return halo


def before_round(pre, dv, lanes):
    if pre is None:
        return (
            jnp.zeros((dv, lanes), F32),
            jnp.ones((1, lanes), F32),
            jnp.zeros((EXTRA_ROWS, lanes), F32),
        )
    return unpack(pre[...], dv)


def join_round(radix, stride, *refs):
    items, pre, (send, pre_out, stack) = refs[:radix], refs[radix:-3], refs[-3:]
    dv = send.shape[0] - EXTRA_ROWS
    fill(stack, items)
    digit = lax.rem(lax.axis_index("sp") // stride, radix)
    lanes = stack.shape[2]
    had_s, had_d, had_halo = before_round(pre[0] if pre else None, dv, lanes)
    pre_s, pre_d = jnp.zeros((dv, lanes), F32), jnp.ones((1, lanes), F32)
    tot_s, tot_d = pre_s, pre_d
    for j in range(radix):
        s, d, tail = unpack(stack[j ^ digit], dv)
        before = j < digit
        pre_s = jnp.where(before, d * pre_s + s, pre_s)
        pre_d = jnp.where(before, d * pre_d, pre_d)
        tot_s, tot_d = d * tot_s + s, d * tot_d
    halo = halo_of_round(had_halo, stack, radix, stride, digit, dv)
    pack(pre_out, had_d * pre_s + had_s, had_d * pre_d, halo)
    pack(send, tot_s, tot_d, tail)


def scaled(x, w, r):
    s = dot(x, w)
    return (s * tile_lanes(r, s.shape[1])).astype(BF16)


def conv_product(full, scale, wc, wh, rows):
    r = scale[rows, :]
    x = full[rows, :]
    p = scaled(x, wc[...], r).astype(F32) * scaled(x, wh[...], r).astype(F32)
    return p.astype(BF16)


def conv_halo(full, scale, wc, wh, send, out):
    rows = full.shape[0]
    p = conv_product(full, scale, wc, wh, slice(rows - 16, rows))
    dv = send.shape[0] - EXTRA_ROWS
    tail = to_tail(p.astype(F32))
    row = lax.broadcasted_iota(jnp.int32, tail.shape, 0)
    out[:dv, :] = send[:dv, :]
    out[dv:, :] = jnp.where(row < 2, send[dv:, :].astype(F32), tail).astype(BF16)


def conv_inputs(full, scale, wc, wh, wg, gain, prod, gate):
    prod[...] = conv_product(full, scale, wc, wh, slice(0, full.shape[0]))
    gated = scaled(full[...], wg[...], scale[...]).astype(F32)
    gate[...] = gated * jax.nn.sigmoid(gated) * tile_lanes(gain[...], gated.shape[1])


def late_half(full, scale, taps, wb, wq, prod, query, outer, conv):
    r = scale[...]
    x = full[...]
    b = scaled(x, wb[...], r)
    outer[...] = b
    p = prod[...].astype(F32)
    row = lax.broadcasted_iota(jnp.int32, p.shape, 0)
    t = taps[...].astype(F32)
    total = jnp.zeros(p.shape, F32)
    for j in range(taps.shape[0] - 1):
        back = taps.shape[0] - 1 - j
        total = total + t[j : j + 1] * jnp.where(row >= back, pltpu.roll(p, back, 0), 0.0)
    total = total + t[taps.shape[0] - 1 :] * p
    conv[...] = (b.astype(F32) * total).astype(BF16)
    query[...] = scaled(x, wq[...], r)


def blockwise(
    key_dim, query, key, val, cum, base, start, raw, through, first
):
    rows = query.shape[0]
    n = rows // BLOCK
    shrink = key_dim**-0.5
    first[...] = start[...].T
    k_mask = block_mask(256, 64, 128, 32)
    v_mask = block_mask(256, 64, 256, 64)
    causal = lax.broadcasted_iota(jnp.int32, (BLOCK, 256), 0) >= (
        lax.broadcasted_iota(jnp.int32, (BLOCK, 256), 1) % BLOCK
    )
    zero = jnp.zeros((), BF16)
    for g in range(val.shape[1] // 256):
        kl = slice(g * 128, (g + 1) * 128)
        vl = slice(g * 256, (g + 1) * 256)
        state = None
        for b in range(n):
            s = slice(b * BLOCK, (b + 1) * BLOCK)
            c = cum[s, kl]
            q = query[s, kl].astype(F32) * shrink
            k = key[s, kl].astype(F32)
            end = c[BLOCK - 1 :]
            grown = q * jnp.exp(c)
            q_in = grown.astype(BF16)
            k_in = (k * jnp.exp(-c)).astype(BF16)
            through[s, kl] = (grown * jnp.exp(base[b : b + 1, kl])).astype(BF16)
            v = val[s, vl]
            k_wide = jnp.where(k_mask, jnp.concatenate([k_in] * 4, axis=0), zero)
            scores = lax.dot_general(q_in, k_wide, NT, preferred_element_type=F32)
            scores = jnp.where(causal, scores, 0.0).astype(BF16)
            v_wide = jnp.where(v_mask, jnp.concatenate([v] * 4, axis=0), zero)
            out = dot(scores, v_wide)
            if state is not None:
                out = out + lax.dot_general(
                    q_in, state.astype(BF16), NT, preferred_element_type=F32
                )
            raw[s, vl] = out
            if b < n - 1:
                k_out = (k * jnp.exp(end - c)).astype(BF16)
                new = lax.dot_general(v, k_out, TN, preferred_element_type=F32)
                new = jnp.where(k_mask, new, 0.0)
                state = new if state is None else state * jnp.exp(end) + new


def rows_out(half, incoming, halo, raw, through, gate, conv, outer, prod, taps):
    rows = raw.shape[0] // 2
    at = pl.multiple_of(half * rows, 64)
    here = pl.ds(at, rows)
    ones = block_mask(256, 64, 256, 64).astype(BF16) * (1.0 / 64)
    ones = ones.astype(BF16)
    parts = []
    for g in range(raw.shape[1] // 256):
        vl = slice(g * 256, (g + 1) * 256)
        x = raw[here, vl] + lax.dot_general(
            through[here, g * 128 : (g + 1) * 128],
            incoming[g],
            NT,
            preferred_element_type=F32,
        )
        mean = dot((x * x).astype(BF16), ones)
        parts.append((x * lax.rsqrt(mean + NORM_EPS) * gate[here, vl]).astype(BF16))
    attn = jnp.concatenate(parts, axis=1)
    p = prod[:16, :].astype(F32)
    row = lax.broadcasted_iota(jnp.int32, p.shape, 0)
    t = taps[...].astype(F32)
    back2 = jnp.where(row == 0, halo[0:1], jnp.where(row == 1, halo[1:2], pltpu.roll(p, 2, 0)))
    back1 = jnp.where(row == 0, halo[1:2], pltpu.roll(p, 1, 0))
    top = outer[:16, :].astype(F32) * (t[0:1] * back2 + t[1:2] * back1 + t[2:3] * p)
    mine = conv[here, :]
    head = jnp.where(half == 0, top, mine[:16].astype(F32)).astype(BF16)
    left = jnp.concatenate([head, mine[16:]], axis=0)
    return left, attn


def project_out(left, attn, wc, wa, out, skip=0):
    step = 512
    for n in range(0, out.shape[1], step):
        at = slice(skip + n, skip + n + step)
        s = dot(left, wc[:, at]) + dot(attn, wa[:, at])
        out[:, n : n + step] = s.astype(out.dtype)


def partner_rows(radix, stride, *refs):
    items, pre = refs[:radix], refs[radix:-16]
    first, raw, through, gate, conv, outer, prod, taps, wc, wa = refs[-16:-6]
    out, left_out, attn_out, state, halo_out, stack = refs[-6:]
    dv = first.shape[0]
    fill(stack, items)
    digit = lax.rem(lax.axis_index("sp") // stride, radix)
    lanes = stack.shape[2]
    had_s, had_d, had_halo = before_round(pre[0] if pre else None, dv, lanes)
    pre_s = first[...]
    for j in range(radix - 1):
        s, d, _ = unpack(stack[j ^ digit], dv)
        pre_s = jnp.where(j < digit, d * pre_s + s, pre_s)
    pre_s = had_d * pre_s + had_s
    mask = block_mask(256, 64, 128, 32)
    incoming = []
    for g in range(lanes // 128):
        s = pre_s[:, g * 128 : (g + 1) * 128]
        wide = jnp.where(mask, jnp.concatenate([s] * 4, axis=0), 0.0).astype(BF16)
        incoming.append(wide)
        state[g] = wide
    halo = from_tail(halo_of_round(had_halo, stack, radix, stride, digit, dv))
    halo_out[...] = jnp.concatenate([halo] * 4, axis=0)
    half = 1 - lax.axis_index("tp")
    left, attn = rows_out(half, incoming, halo, raw, through, gate, conv, outer, prod, taps)
    left_out[...] = left
    attn_out[...] = attn
    project_out(left, attn, wc, wa, out)


def partner_rest(left, attn, wc, wa, out):
    project_out(left[...], attn[...], wc, wa, out, out.shape[1])


def add_rows(mine, first, second, out_hbm, buf, sems):
    chunks = buf.shape[0]
    rows = buf.shape[1]
    width = first.shape[1]
    copies = []
    for i in range(chunks):
        here = slice(i * rows, (i + 1) * rows)
        buf[i, :, :width] = (mine[here, :width] + first[here, :].astype(F32)).astype(BF16)
        buf[i, :, width:] = (mine[here, width:] + second[here, :].astype(F32)).astype(BF16)
        copies.append(pltpu.make_async_copy(buf.at[i], out_hbm.at[here, :], sems.at[i]))
        copies[-1].start()
    for c in copies:
        c.wait()


def own_rows(state, halo, raw, through, gate, conv, outer, prod, taps, wc, wa, out):
    incoming = [state[g] for g in range(state.shape[0])]
    half = lax.axis_index("tp")
    left, attn = rows_out(
        half, incoming, halo[0:2, :], raw, through, gate, conv, outer, prod, taps
    )
    project_out(left, attn, wc, wa, out)


def radices(n):
    found = []
    while n > 1:
        r = 4 if n % 4 == 0 else 2
        found.append(r)
        n //= r
    return found


def on_device(
    tokens,
    input_norm_gain,
    outer_gate_weight,
    inner_gate_weight,
    convolution_input_weight,
    convolution_kernel_taps,
    query_weight_matrix,
    key_weight_matrix,
    value_weight_matrix,
    forget_gate_weight,
    attention_gate_weight,
    forget_gate_bias,
    extra_logarithm_decay,
    initial_head_state,
    head_norm_gain,
    convolution_output_weight,
    attention_output_weight,
):
    rows, half = tokens.shape
    heads, dk, dv = initial_head_state.shape
    kw, vw, cw = heads * dk, heads * dv, outer_gate_weight.shape[1]
    model = convolution_output_weight.shape[1]
    n_sp = lax.axis_size("sp")
    swap = [(0, 1), (1, 0)]
    other = lax.ppermute(tokens, "tp", swap)
    gain = input_norm_gain.reshape(1, -1)
    early = (key_weight_matrix, forget_gate_weight, value_weight_matrix)
    width = sum(w.shape[1] for w in early)
    extra = extra_logarithm_decay.T
    flops = 2 * rows * half * width
    acc, xg, ssq, wide, ahead = call(
        own_half,
        [
            ((rows, width), F32),
            ((rows, half), BF16),
            ((rows, 128), F32),
            ((rows, kw), F32),
            ((half, width), BF16),
        ],
        [(tokens, HBM), (gain, HBM), (extra, HBM)] + [(w, HBM) for w in early],
        flops,
        [
            pltpu.VMEM((half, width), BF16),
            pltpu.SemaphoreType.DMA((2, len(early))),
            pltpu.VMEM(tokens.shape, BF16),
            pltpu.VMEM(gain.shape, F32),
            pltpu.VMEM(extra.shape, F32),
            pltpu.SemaphoreType.DMA((3,)),
        ],
    )
    full, scale, key, val, cum, base, send = call(
        other_half,
        [
            ((rows, 2 * half), BF16),
            ((rows, 128), F32),
            ((rows, kw), BF16),
            ((rows, vw), BF16),
            ((rows, kw), F32),
            ((8, kw), F32),
            ((dv + EXTRA_ROWS, kw), BF16),
        ],
        [(other, VMEM), (gain, VMEM), (forget_gate_bias.reshape(1, -1), VMEM)]
        + [(a, VMEM) for a in (acc, xg, ssq, wide, ahead)],
        flops,
    )
    (send_halo,) = call(
        conv_halo,
        [(send.shape, BF16)],
        [(a, VMEM) for a in (full, scale, inner_gate_weight, convolution_input_weight, send)],
        2 * rows * half * cw,
    )
    prod, gate = call(
        conv_inputs,
        [((rows, cw), BF16), ((rows, vw), F32)],
        [
            (a, VMEM)
            for a in (
                full,
                scale,
                inner_gate_weight,
                convolution_input_weight,
                attention_gate_weight,
                head_norm_gain.reshape(1, -1),
            )
        ],
        2 * rows * 2 * half * (2 * cw + vw),
    )
    query, outer, conv = call(
        late_half,
        [((rows, kw), BF16), ((rows, cw), BF16), ((rows, cw), BF16)],
        [
            (a, VMEM)
            for a in (
                full,
                scale,
                convolution_kernel_taps,
                outer_gate_weight,
                query_weight_matrix,
                prod,
            )
        ],
        2 * rows * 2 * half * (kw + cw),
    )
    raw, through, first = call(
        functools.partial(blockwise, dk),
        [((rows, vw), F32), ((rows, kw), BF16), ((dv, kw), F32)],
        [
            (a, VMEM)
            for a in (query, key, val, cum, base, initial_head_state.reshape(heads * dk, dv))
        ],
        1 << 24,
    )
    pre = ()
    stride = 1
    plan = radices(n_sp)
    crossed = len(plan) % 2 == 0
    for turn, radix in enumerate(plan):
        items = [send] + [None] * (radix - 1)
        for j in FIRST if turn == 0 else LAST if radix == 4 else range(1, radix):
            pairs = [
                (2 * i + c, 2 * (i ^ (j * stride)) + (1 - c if crossed else c))
                for i in range(n_sp)
                for c in range(2)
            ]
            payload = send_halo if turn == 0 and j % 2 == 1 else send
            items[j] = lax.ppermute(payload, ("sp", "tp"), pairs)
        if crossed and turn < len(plan) - 1:
            items[0] = lax.ppermute(send, "tp", swap)
        if crossed and turn > 0:
            pre = (lax.ppermute(pre[0], "tp", swap),)
        stack = [pltpu.VMEM((radix,) + send.shape, BF16)]
        if turn < len(plan) - 1:
            send, *pre = call(
                functools.partial(join_round, radix, stride),
                [(send.shape, BF16), (send.shape, BF16)],
                [(a, VMEM) for a in (*items, *pre)],
                1 << 20,
                stack,
            )
            stride *= radix
    tail = [
        (a, VMEM)
        for a in (
            raw,
            through,
            gate,
            conv,
            outer,
            prod,
            convolution_kernel_taps,
            convolution_output_weight,
            attention_output_weight,
        )
    ]
    flops = 2 * (rows // 2) * model * (vw + cw)
    theirs, left, attn, state, halo = call(
        functools.partial(partner_rows, plan[-1], stride),
        [
            ((rows // 2, model // 2), BF16),
            ((rows // 2, cw), BF16),
            ((rows // 2, vw), BF16),
            ((kw // 128, 256, 128), BF16),
            ((8, cw), F32),
        ],
        [(a, VMEM) for a in (*items, *pre, first)] + tail,
        flops // 2,
        stack,
    )
    got_first = lax.ppermute(theirs, "tp", swap)
    (theirs,) = call(
        partner_rest,
        [((rows // 2, model // 2), BF16)],
        [
            (a, VMEM)
            for a in (left, attn, convolution_output_weight, attention_output_weight)
        ],
        flops // 2,
    )
    got_second = lax.ppermute(theirs, "tp", swap)
    (mine,) = call(
        own_rows, [((rows // 2, model), F32)], [(state, VMEM), (halo, VMEM)] + tail, flops
    )
    return pl.pallas_call(
        add_rows,
        out_shape=jax.ShapeDtypeStruct((rows // 2, model), BF16),
        in_specs=[VMEM] * 3,
        out_specs=HBM,
        scratch_shapes=[
            pltpu.VMEM((CHUNKS, rows // 2 // CHUNKS, model), BF16),
            pltpu.SemaphoreType.DMA((CHUNKS,)),
        ],
        compiler_params=pltpu.CompilerParams(vmem_limit_bytes=12 << 20),
        cost_estimate=pl.CostEstimate(flops=1 << 20, bytes_accessed=1 << 20, transcendentals=0),
        name="add_rows",
    )(mine, got_first, got_second)


def solution(mesh):
    placed = (
        P("sp", "tp"),
        P(),
        P(None, "tp"),
        P(None, "tp"),
        P(None, "tp"),
        P(None, "tp"),
        P(None, "tp"),
        P(None, "tp"),
        P(None, "tp"),
        P(None, "tp"),
        P(None, "tp"),
        P("tp"),
        P("sp", "tp"),
        P("tp", None, None),
        P(),
        P("tp", None),
        P("tp", None),
    )

    return jax.shard_map(
        on_device, mesh=mesh, in_specs=placed, out_specs=P(("sp", "tp"), None), check_vma=False
    )
```
